256 devices in a mesh: sp: 64 (over z, x, core), tp: 4 (over y).
Axes of the slice: x: 4, y: 4, z: 8, core: 2. Of those that a mesh axis runs over, the one named last changes fastest.
Arguments:
- layer_input: bfloat16 [10240, 4096], P('sp', 'tp'), may hold values from -24 to 24
- output_grad: bfloat16 [10240, 4096], P('sp', 'tp'), may hold values from -64 to 64
- query_weight: bfloat16 [4096, 2048], P(None, 'tp'), may hold values from -0.09375 to 0.09375
- key_weight: bfloat16 [4096, 1024], P(None, 'tp'), may hold values from -0.09375 to 0.09375
- value_weight: bfloat16 [4096, 1024], P(None, 'tp'), may hold values from -0.09375 to 0.09375
- out_weight: bfloat16 [2048, 4096], P('tp'), may hold values from -0.125 to 0.125
- sink_logit: float32 [16], P('tp'), may hold values from 3 to 7
Outputs:
- input_grad: bfloat16 [10240, 4096], P('sp', 'tp')
- query_weight_grad: float32 [4096, 2048], P('sp', 'tp')
- key_weight_grad: float32 [4096, 1024], P('sp', 'tp')
- value_weight_grad: float32 [4096, 1024], P('sp', 'tp')
- out_weight_grad: float32 [2048, 4096], P('tp', 'sp')
- sink_grad: float32 [16], P('tp')
The draws below stay inside these ranges and needn't reach their ends.
All inputs are finite; a program needn't handle non-finite values.
Results may differ from the reference program's by a relative error of at most 0.015.
Values may be sent and summed in bfloat16 or wider, within the bound.
A program may use at most 192 MiB of HBM per device.

```python
import jax
import jax.numpy as jnp
from jax import lax

D = 4096
HEADS = 16
KV_HEADS = 8
HEAD = 128
WINDOW = 128
TOK_DEV = 160
TOKENS = 10240


def draw_layer_input(key, part):
    key_normal = jax.random.fold_in(key, 11)
    key_pairing = jax.random.fold_in(key, 12)
    normal_part = jnp.clip(jax.random.normal(key_normal, (TOKENS, D), jnp.float32), -4.0, 4.0)
    blocks = TOKENS // TOK_DEV
    pairing = jax.random.permutation(key_pairing, blocks)
    row_block = jnp.arange(TOKENS, dtype=jnp.int32) // TOK_DEV
    col_block = jnp.arange(D, dtype=jnp.int32) * blocks // D
    spiked = pairing[row_block][:, None] == col_block[None, :]
    values = normal_part * jnp.where(spiked, 3.0, 1.0)
    return values.astype(jnp.bfloat16)


def strengthened(entries, own_key, source, target, parts, factor):
    owner, partner = [(jnp.arange(entries.shape[axis_at]) // (entries.shape[axis_at] // parts)).reshape([-1 if axis == axis_at else 1 for axis in range(entries.ndim)]) for axis_at in (source, target)]
    chosen = jax.random.permutation(own_key, parts)[partner]
    strong = (owner == chosen) | (owner == (partner + parts // 2) % parts)
    return jnp.where(strong, factor * entries, entries)


def block_levels(stream_key, shape, cuts, smallest, largest):
    def one(dim, shards_of):
        draws = jax.random.uniform(jax.random.fold_in(jax.random.fold_in(stream_key, 6), dim), (shards_of,), jnp.float32, smallest / len(cuts), largest / len(cuts))
        return jnp.repeat(jnp.exp(draws), shape[dim] // shards_of).reshape((-1,) + (1,) * (len(shape) - dim - 1))

    level = one(*cuts[0])
    for cut in cuts[1:]:
        level = level * one(*cut)
    return level


def scatter_about(key, shape, deviation, limit, pieces=(), kind=jnp.bfloat16):
    entries = jax.random.normal(key, shape, jnp.float32) * deviation
    if len(pieces) > 0:
        entries = block_levels(key, shape, pieces, -0.22, 0.18) * entries
    return jnp.clip(entries, min=-limit, max=limit).astype(kind)


def bell_draw_with(stream_key, shape, deviation, bound, pieces, heavy, kind=jnp.bfloat16):
    entries = deviation * jax.random.normal(stream_key, shape, jnp.float32)
    if pieces:
        entries = entries * block_levels(stream_key, shape, pieces, -0.22, 0.18)
    return jnp.clip(strengthened(entries, jax.random.fold_in(stream_key, 3), *heavy), -bound, bound).astype(kind)


def setup_inputs(seed: int = 0) -> dict:
    key_list = jax.random.split(jax.random.key(seed), 8)
    return {
        "layer_input": draw_layer_input(jax.random.fold_in(key_list[7], 71), 0),
        "output_grad": bell_draw_with(key_list[1], (TOKENS, D), 4.0, 64.0, ((0, 64), (1, 4)), (0, 1, 64, 4.0)),
        "query_weight": scatter_about(key_list[2], (D, HEADS * HEAD), D ** -0.5, 0.09375, ((1, 4),)),
        "key_weight": scatter_about(key_list[3], (D, KV_HEADS * HEAD), D ** -0.5, 0.09375, ((1, 4),)),
        "value_weight": scatter_about(key_list[4], (D, KV_HEADS * HEAD), D ** -0.5, 0.09375, ((1, 4),)),
        "out_weight": scatter_about(key_list[5], (HEADS * HEAD, D), (HEADS * HEAD) ** -0.5, 0.125, ((0, 4),)),
        "sink_logit": jnp.clip(3.0 + 4.0 * jax.random.uniform(key_list[6], (HEADS,), jnp.float32) ** block_levels(key_list[6], (HEADS,), ((0, 4),), -0.2, 0.2), 3.0, 7.0),
    }


masked_score = -1e30


def reference(layer_input, output_grad, query_weight, key_weight, value_weight, out_weight, sink_logit):
    seq_len = layer_input.shape[0]
    group_size = HEADS // KV_HEADS
    scaling = HEAD ** -0.5
    block_count = seq_len // WINDOW
    queries = jnp.dot(layer_input, query_weight, preferred_element_type=jnp.float32).astype(jnp.bfloat16)
    queries = queries.reshape(seq_len, KV_HEADS, group_size, HEAD)
    key_rows = jnp.dot(layer_input, key_weight, preferred_element_type=jnp.float32).astype(jnp.bfloat16)
    key_rows = key_rows.reshape(seq_len, KV_HEADS, HEAD)
    value_rows = jnp.dot(layer_input, value_weight, preferred_element_type=jnp.float32).astype(jnp.bfloat16)
    value_rows = value_rows.reshape(seq_len, KV_HEADS, HEAD)
    out_rows_grad = jnp.dot(output_grad, out_weight.T, preferred_element_type=jnp.float32).astype(jnp.bfloat16)
    out_rows_grad = out_rows_grad.reshape(seq_len, KV_HEADS, group_size, HEAD)
    sink_column = sink_logit.astype(jnp.float32).reshape(KV_HEADS, group_size)[:, :, None]
    edge_three = ((WINDOW, WINDOW), (0, 0), (0, 0))
    edge_four = ((WINDOW, WINDOW), (0, 0), (0, 0), (0, 0))
    padded_keys = jnp.pad(key_rows, edge_three)
    padded_values = jnp.pad(value_rows, edge_three)

    def forward_block(block):
        offset = block * WINDOW
        query_block = lax.dynamic_slice_in_dim(queries, offset, WINDOW, 0).astype(jnp.float32)
        grad_block = lax.dynamic_slice_in_dim(out_rows_grad, offset, WINDOW, 0).astype(jnp.float32)
        key_band = lax.dynamic_slice_in_dim(padded_keys, offset, 3 * WINDOW, 0).astype(jnp.float32)
        value_band = lax.dynamic_slice_in_dim(padded_values, offset, 3 * WINDOW, 0).astype(jnp.float32)
        query_pos = offset + jnp.arange(WINDOW, dtype=jnp.int32)
        key_pos = offset - WINDOW + jnp.arange(3 * WINDOW, dtype=jnp.int32)
        in_window = (jnp.abs(query_pos[:, None] - key_pos[None, :]) <= WINDOW) & (key_pos[None, :] >= 0) & (key_pos[None, :] < seq_len)
        scores = jnp.einsum("qkgd,skd->kgqs", query_block, key_band) * scaling
        scores = jnp.where(in_window[None, None], scores, masked_score)
        row_max = jnp.maximum(jnp.max(scores, axis=-1), sink_column)
        row_total = jnp.sum(jnp.exp(scores - row_max[..., None]), axis=-1) + jnp.exp(sink_column - row_max)
        log_total = row_max + jnp.log(row_total)
        soft_weights = jnp.exp(scores - log_total[..., None])
        soft_rounded = soft_weights.astype(jnp.bfloat16)
        attended = jnp.einsum("kgqs,skd->qkgd", soft_rounded.astype(jnp.float32), value_band).astype(jnp.bfloat16)
        row_dots = jnp.sum(grad_block * attended.astype(jnp.float32), axis=-1)
        dots_moved = row_dots.transpose(1, 2, 0)
        prob_grads = jnp.einsum("qkgd,skd->kgqs", grad_block, value_band)
        score_grads = (soft_weights * (prob_grads - dots_moved[..., None])).astype(jnp.bfloat16)
        query_grads = (jnp.einsum("kgqs,skd->qkgd", score_grads.astype(jnp.float32), key_band) * scaling).astype(jnp.bfloat16)
        sink_part = -jnp.sum(jnp.exp(sink_column - log_total) * dots_moved, axis=-1)
        return attended, log_total, row_dots, query_grads, sink_part

    attended, log_total, row_dots, query_grads, sink_parts = lax.map(forward_block, jnp.arange(block_count, dtype=jnp.int32))
    attended = attended.reshape(seq_len, HEADS * HEAD)
    log_total = log_total.transpose(0, 3, 1, 2).reshape(seq_len, KV_HEADS, group_size)
    row_dots = row_dots.reshape(seq_len, KV_HEADS, group_size)
    query_grads = query_grads.reshape(seq_len, HEADS * HEAD)
    sink_grad = jnp.sum(sink_parts, axis=0).reshape(HEADS)
    padded_queries = jnp.pad(queries, edge_four)
    padded_out_grad = jnp.pad(out_rows_grad, edge_four)
    padded_totals = jnp.pad(log_total, edge_three)
    padded_dots = jnp.pad(row_dots, edge_three)

    def key_block(block):
        offset = block * WINDOW
        key_own = lax.dynamic_slice_in_dim(key_rows, offset, WINDOW, 0).astype(jnp.float32)
        value_own = lax.dynamic_slice_in_dim(value_rows, offset, WINDOW, 0).astype(jnp.float32)
        query_band = lax.dynamic_slice_in_dim(padded_queries, offset, 3 * WINDOW, 0).astype(jnp.float32)
        grad_band = lax.dynamic_slice_in_dim(padded_out_grad, offset, 3 * WINDOW, 0).astype(jnp.float32)
        total_band = lax.dynamic_slice_in_dim(padded_totals, offset, 3 * WINDOW, 0).transpose(1, 2, 0)
        dots_band = lax.dynamic_slice_in_dim(padded_dots, offset, 3 * WINDOW, 0).transpose(1, 2, 0)
        query_pos = offset - WINDOW + jnp.arange(3 * WINDOW, dtype=jnp.int32)
        key_pos = offset + jnp.arange(WINDOW, dtype=jnp.int32)
        in_window = (jnp.abs(query_pos[:, None] - key_pos[None, :]) <= WINDOW) & (query_pos[:, None] >= 0) & (query_pos[:, None] < seq_len)
        scores = jnp.einsum("qkgd,skd->kgqs", query_band, key_own) * scaling
        scores = jnp.where(in_window[None, None], scores, masked_score)
        soft_weights = jnp.exp(scores - total_band[..., None])
        soft_rounded = soft_weights.astype(jnp.bfloat16)
        prob_grads = jnp.einsum("qkgd,skd->kgqs", grad_band, value_own)
        score_grads = (soft_weights * (prob_grads - dots_band[..., None])).astype(jnp.bfloat16)
        key_grads = (jnp.einsum("kgqs,qkgd->skd", score_grads.astype(jnp.float32), query_band) * scaling).astype(jnp.bfloat16)
        value_grads = jnp.einsum("kgqs,qkgd->skd", soft_rounded.astype(jnp.float32), grad_band).astype(jnp.bfloat16)
        return key_grads, value_grads

    key_grads, value_grads = lax.map(key_block, jnp.arange(block_count, dtype=jnp.int32))
    key_grads = key_grads.reshape(seq_len, KV_HEADS * HEAD)
    value_grads = value_grads.reshape(seq_len, KV_HEADS * HEAD)
    input_grad = (jnp.dot(query_grads, query_weight.T, preferred_element_type=jnp.float32)
                  + jnp.dot(key_grads, key_weight.T, preferred_element_type=jnp.float32)
                  + jnp.dot(value_grads, value_weight.T, preferred_element_type=jnp.float32)).astype(jnp.bfloat16)
    query_weight_grad = jnp.dot(layer_input.T, query_grads, preferred_element_type=jnp.float32)
    key_weight_grad = jnp.dot(layer_input.T, key_grads, preferred_element_type=jnp.float32)
    value_weight_grad = jnp.dot(layer_input.T, value_grads, preferred_element_type=jnp.float32)
    out_weight_grad = jnp.dot(attended.T, output_grad, preferred_element_type=jnp.float32)
    return (input_grad, query_weight_grad, key_weight_grad, value_weight_grad, out_weight_grad, sink_grad)
```

```python
import jax
import jax.numpy as jnp
from jax import lax
from jax.experimental import pallas as pl
from jax.experimental.pallas import tpu as pltpu
from jax.sharding import PartitionSpec as P

HEAD = 128
WINDOW = 128
NZ, NX, NC, NY = 8, 4, 2, 4
TOK = 160
SEQ = TOK * NZ * NX * NC
BAND = TOK + 2 * WINDOW
QC = 512
KC = 256
SCALING = HEAD ** (-0.5)
MASKED = -1e30
BF = jnp.bfloat16
F32 = jnp.float32
COPIES = 160


def mm(left, right, left_dim, right_dim):
    return lax.dot_general(
        left, right, (((left_dim,), (right_dim,)), ((), ())), preferred_element_type=F32
    )


def kernel(
    x_hbm, g_hbm, wq_hbm, wk_hbm, wv_hbm, wo_hbm, sink_ref,
    dx_out, wq_out, wk_out, wv_out, wo_out, sink_out,
    xg, dg, xc, dc, rx, rd, wq, wk, wv, wo, acc, dacc, band, queries, grads,
    soft, psink, gc, kvg, hs, hr, pf, pb, sr, zs, zr, ys, yr, yrelay, dxo, skx, skc, skz,
    local_sem, send_sem, recv_sem,
):
    sp = lax.axis_index("sp")
    y = lax.axis_index("tp")
    z = sp // (NX * NC)
    x = lax.rem(sp // NC, NX)
    c = lax.rem(sp, NC)

    def at_y(step):
        return (sp, lax.rem(y + step, NY))

    def at_x(step):
        return ((z * NX + lax.rem(x + step, NX)) * NC + c, y)

    def at_z(step):
        return ((lax.rem(z + step, NZ) * NX + x) * NC + c, y)

    sister = (sp + 1 - 2 * c, y)
    after = (lax.rem(sp + 1, NZ * NX * NC), y)
    before = (lax.rem(sp + NZ * NX * NC - 1, NZ * NX * NC), y)
    up, down = at_y(1), at_y(3)
    right, left = at_x(1), at_x(3)

    started = []
    local_count = [0]

    def send(src, dst, device):
        k = len(started)
        copy = pltpu.make_async_remote_copy(
            src_ref=src,
            dst_ref=dst,
            send_sem=send_sem.at[k],
            recv_sem=recv_sem.at[k],
            device_id=device,
            device_id_type=pl.DeviceIdType.MESH,
        )
        copy.start()
        started.append(copy)
        return copy

    def load(src, dst):
        k = local_count[0]
        local_count[0] += 1
        copy = pltpu.make_async_copy(src, dst, local_sem.at[k])
        copy.start()
        return copy

    def loads(hbm, blocks):
        return [
            [
                load(hbm.at[:, pl.ds((h * 4 + k) * 128, 128)], blocks.at[0, h, k])
                for k in range(4)
            ]
            for h in range(2)
        ]

    x_loads = loads(x_hbm, xg)
    weight_loads = [load(wq_hbm, wq), load(wk_hbm, wk), load(wv_hbm, wv)]
    d_loads = loads(g_hbm, dg)
    out_load = load(wo_hbm, wo)

    barrier = pltpu.get_barrier_semaphore()
    peers = [up, down, right, left, at_x(2), sister, after, before]
    peers += [at_z(step) for step in range(1, NZ)]
    for peer in peers:
        pl.semaphore_signal(
            barrier, inc=1, device_id=peer, device_id_type=pl.DeviceIdType.MESH
        )
    pl.semaphore_wait(barrier, len(peers))

    def gather_start(blocks):
        return (
            send(blocks.at[0, 0], blocks.at[1, 0], up),
            send(blocks.at[0, 1], blocks.at[3, 1], down),
            send(blocks.at[0, 1], blocks.at[1, 1], up),
            send(blocks.at[0, 0], blocks.at[3, 0], down),
        )

    def gather_pass(blocks, first):
        first[0].wait_recv()
        a = send(blocks.at[1, 0], blocks.at[2, 0], up)
        first[1].wait_recv()
        b = send(blocks.at[3, 1], blocks.at[2, 1], down)
        return a, b

    def exchange(blocks, cells, relay, ry):
        xr, xo, xl = lax.rem(x + 1, NX), lax.rem(x + 2, NX), lax.rem(x + 3, NX)
        near = (
            send(blocks.at[ry, :, xr], cells.at[ry, :, 1], right),
            send(blocks.at[ry, :, xl], cells.at[ry, :, 3], left),
        )
        far = (
            send(blocks.at[ry, 0, xo], relay.at[ry, 0], right),
            send(blocks.at[ry, 1, xo], relay.at[ry, 1], left),
        )
        for h in range(2):
            cells[ry, h, 0] = blocks[ry, h, x]
        return near, far

    def exchange_pass(cells, relay, ry, far):
        far[0].wait_recv()
        a = send(relay.at[ry, 0], cells.at[ry, 0, 2], right)
        far[1].wait_recv()
        b = send(relay.at[ry, 1], cells.at[ry, 1, 2], left)
        return a, b

    def wide(blocks, ry):
        return jnp.concatenate([blocks[ry, h, k] for h in range(2) for k in range(4)], axis=1)

    def features(ry):
        return pl.multiple_of(lax.rem(y + NY - ry, NY) * 1024, 1024)

    def project(ry):
        rows = pl.ds(features(ry), 1024)
        block = wide(xg, ry)
        for cols, weight in (
            (slice(0, QC), wq),
            (slice(QC, QC + KC), wk),
            (slice(QC + KC, QC + 2 * KC), wv),
        ):
            term = mm(block, weight[rows, :], 1, 0)
            acc[:, cols] = term if ry == 0 else acc[:, cols] + term

    def project_grad(ry):
        cols = pl.ds(features(ry), 1024)
        term = mm(wide(dg, ry), wo[:, cols], 1, 1)
        dacc[...] = term if ry == 0 else dacc[...] + term

    for half in x_loads:
        for copy in half:
            copy.wait()
    x_first = gather_start(xg)
    x_ex = {0: exchange(xg, xc, rx, 0)}
    for copy in weight_loads:
        copy.wait()
    project(0)
    x_second = gather_pass(xg, x_first)
    for half in d_loads:
        for copy in half:
            copy.wait()
    d_first = gather_start(dg)
    x_passed = [exchange_pass(xc, rx, 0, x_ex[0][1])]
    x_first[2].wait_recv()
    x_ex[1] = exchange(xg, xc, rx, 1)
    x_first[3].wait_recv()
    x_ex[3] = exchange(xg, xc, rx, 3)
    project(1)
    project(3)
    for copy in x_second:
        copy.wait_recv()
    x_ex[2] = exchange(xg, xc, rx, 2)
    project(2)

    band[WINDOW : WINDOW + TOK, :] = acc[:, QC : QC + 2 * KC].astype(BF)
    queries[...] = acc[:, :QC].astype(BF)
    halo_after = send(band.at[pl.ds(TOK, WINDOW)], band.at[pl.ds(0, WINDOW)], after)
    halo_before = send(
        band.at[pl.ds(WINDOW, WINDOW)], band.at[pl.ds(WINDOW + TOK, WINDOW)], before
    )
    d_second = gather_pass(dg, d_first)
    for ry in (1, 3):
        x_passed.append(exchange_pass(xc, rx, ry, x_ex[ry][1]))
    out_load.wait()
    d_ex = {0: exchange(dg, dc, rd, 0)}
    project_grad(0)
    halo_after.wait_recv()
    halo_before.wait_recv()

    row = lax.broadcasted_iota(jnp.int32, (2 * TOK, BAND), 0)
    row = jnp.where(row >= TOK, row - TOK, row)
    col = lax.broadcasted_iota(jnp.int32, (2 * TOK, BAND), 1) - WINDOW
    key_pos = sp * TOK + col
    in_window = (jnp.abs(row - col) <= WINDOW) & (key_pos >= 0) & (key_pos < SEQ)
    second_head = lax.broadcasted_iota(jnp.int32, (2 * TOK, 1), 0) >= TOK

    def heads(ref, kh):
        cols = kh * 2 * HEAD
        return jnp.concatenate(
            [ref[:, cols : cols + HEAD], ref[:, cols + HEAD : cols + 2 * HEAD]], axis=0
        )

    def put_heads(group, kh, value):
        cols = kh * 2 * HEAD
        gc[group, 0, :, cols : cols + HEAD] = value[:TOK].astype(BF)
        gc[group, 0, :, cols + HEAD : cols + 2 * HEAD] = value[TOK:].astype(BF)

    for kh in range(2):
        keys = band[:, kh * HEAD : (kh + 1) * HEAD]
        values = band[:, KC + kh * HEAD : KC + (kh + 1) * HEAD]
        scores = mm(heads(queries, kh), keys, 1, 1) * SCALING
        scores = jnp.where(in_window, scores, MASKED)
        sink = jnp.where(second_head, sink_ref[2 * kh + 1], sink_ref[2 * kh])
        row_max = jnp.maximum(jnp.max(scores, axis=1, keepdims=True), sink)
        weights = jnp.exp(scores - row_max)
        sink_weight = jnp.exp(sink - row_max)
        inverse = 1.0 / (jnp.sum(weights, axis=1, keepdims=True) + sink_weight)
        weights = weights * inverse
        soft[kh] = weights
        psink[kh] = sink_weight * inverse
        put_heads(0, kh, mm(weights.astype(BF), values, 1, 0))

    half = TOK // 2

    def share(group):
        own = gc.at[group, 0]
        low, high = pl.ds(0, half), pl.ds(half, half)
        return (
            send(own.at[low], gc.at[group, 1, low], right),
            send(own.at[high], gc.at[group, 3, high], left),
            send(own.at[high], gc.at[group, 1, high], right),
            send(own.at[low], gc.at[group, 3, low], left),
        )

    def share_pass(group, first):
        low, high = pl.ds(0, half), pl.ds(half, half)
        first[0].wait_recv()
        a = send(gc.at[group, 1, low], gc.at[group, 2, low], right)
        first[1].wait_recv()
        b = send(gc.at[group, 3, high], gc.at[group, 2, high], left)
        return a, b

    def arrived(first, second):
        for copy in first[2:] + second:
            copy.wait_recv()

    att_first = share(0)
    x_passed.append(exchange_pass(xc, rx, 2, x_ex[2][1]))
    d_passed = [exchange_pass(dc, rd, 0, d_ex[0][1])]
    d_first[2].wait_recv()
    d_ex[1] = exchange(dg, dc, rd, 1)
    d_first[3].wait_recv()
    d_ex[3] = exchange(dg, dc, rd, 3)
    project_grad(1)
    project_grad(3)
    att_second = share_pass(0, att_first)
    for copy in d_second:
        copy.wait_recv()
    d_ex[2] = exchange(dg, dc, rd, 2)
    project_grad(2)
    grads[...] = dacc[...].astype(BF)

    lane = lax.broadcasted_iota(jnp.int32, (8, 128), 1)
    sink_tile = jnp.zeros((8, 128), F32)
    for kh in range(2):
        keys = band[:, kh * HEAD : (kh + 1) * HEAD]
        values = band[:, KC + kh * HEAD : KC + (kh + 1) * HEAD]
        query = heads(queries, kh)
        grad = heads(grads, kh)
        attended = heads(gc.at[0, 0], kh)
        row_dots = jnp.sum(grad.astype(F32) * attended.astype(F32), axis=1, keepdims=True)
        weights = soft[kh]
        prob_grads = mm(grad, values, 1, 1)
        score_grads = (weights * (prob_grads - row_dots)).astype(BF)
        put_heads(1, kh, mm(score_grads, keys, 1, 0) * SCALING)
        kvg[:, kh * HEAD : (kh + 1) * HEAD] = mm(score_grads, query, 0, 0) * SCALING
        kvg[:, KC + kh * HEAD : KC + (kh + 1) * HEAD] = mm(weights.astype(BF), grad, 0, 0)
        sink_rows = psink[kh] * row_dots
        for g in range(2):
            total = -jnp.sum(sink_rows[g * TOK : (g + 1) * TOK], axis=0, keepdims=True)
            sink_tile = jnp.where(lane == 2 * kh + g, total, sink_tile)
    hs[0] = kvg[0:WINDOW, :].astype(BF)
    hs[1] = kvg[WINDOW + TOK : BAND, :].astype(BF)
    back = send(hs.at[0], hr.at[0], before)
    forth = send(hs.at[1], hr.at[1], after)
    q_first = share(1)
    skx[x] = sink_tile
    sink_x = [send(skx.at[x], skx.at[x], at_x(step)) for step in (1, 3, 2)]

    for ry in (1, 3):
        d_passed.append(exchange_pass(dc, rd, ry, d_ex[ry][1]))
    back.wait_recv()
    forth.wait_recv()
    kvg[WINDOW + TOK - WINDOW : WINDOW + TOK, :] += hr[0].astype(F32)
    kvg[WINDOW : 2 * WINDOW, :] += hr[1].astype(F32)
    gc[2, 0] = kvg[WINDOW : WINDOW + TOK, :].astype(BF)
    k_first = share(2)
    d_passed.append(exchange_pass(dc, rd, 2, d_ex[2][1]))
    q_second = share_pass(1, q_first)

    def input_share(step):
        rows = pl.ds(pl.multiple_of(lax.rem(y + step, NY) * 1024, 1024), 1024)
        return (
            mm(gc[1, 0], wq[rows, :], 1, 1)
            + mm(gc[2, 0, :, :KC], wk[rows, :], 1, 1)
            + mm(gc[2, 0, :, KC:], wv[rows, :], 1, 1)
        )

    ys[1] = input_share(2).astype(BF)
    y_far = (
        send(ys.at[1, pl.ds(0, half)], yrelay.at[0], up),
        send(ys.at[1, pl.ds(half, half)], yrelay.at[1], down),
    )
    ys[0] = input_share(1).astype(BF)
    y_near = [send(ys.at[0], yr.at[0], up)]
    ys[2] = input_share(3).astype(BF)
    y_near.append(send(ys.at[2], yr.at[2], down))
    k_second = share_pass(2, k_first)
    dxo[...] = input_share(0)

    for near, _ in list(x_ex.values()) + list(d_ex.values()):
        for copy in near:
            copy.wait_recv()
    for pair in x_passed + d_passed:
        for copy in pair:
            copy.wait_recv()
    for copy in sink_x:
        copy.wait_recv()
    skc[c] = (skx[0] + skx[1]) + (skx[2] + skx[3])
    sink_c = send(skc.at[c], skc.at[c], sister)

    def multiply(group, cells):
        rows = jnp.concatenate(
            [cells[ry, h].reshape(NX * TOK, 128) for ry in range(NY) for h in range(2)], axis=1
        )
        product = mm(rows, gc[group].reshape(NX * TOK, QC), 0, 0)
        product = product.reshape(NY, 2, NC, 64, QC)
        pf[group] = product
        pb[group] = product.astype(BF)
        return send(pb.at[group, :, :, 1 - c], sr.at[group], sister)

    def spread(group, from_sister):
        from_sister.wait_recv()
        for ry in range(NY):
            for h in range(2):
                zs[group, ry, h] = (pf[group, ry, h, c] + sr[group, ry, h].astype(F32)).astype(BF)
        copies = []
        for step in (4, 3, 5, 2, 6, 1, 7):
            to = lax.rem(z + step, NZ)
            ry = lax.rem(y + NY - to // 2, NY)
            copies.append(send(zs.at[group, ry, lax.rem(to, 2)], zr.at[group, step - 1], at_z(step)))
        return copies

    def collect(group, copies):
        ry = lax.rem(y + NY - z // 2, NY)
        h = lax.rem(z, 2)
        total = pf[group, ry, h, c] + sr[group, ry, h].astype(F32)
        for copy in copies:
            copy.wait_recv()
        for step in range(1, NZ):
            total = total + zr[group, step - 1].astype(F32)
        return total

    arrived(att_first, att_second)
    s0 = multiply(0, dc)
    y_far[0].wait_recv()
    y_pass = [send(yrelay.at[0], yr.at[1, pl.ds(0, half)], up)]
    y_far[1].wait_recv()
    y_pass.append(send(yrelay.at[1], yr.at[1, pl.ds(half, half)], down))
    arrived(q_first, q_second)
    s1 = multiply(1, xc)
    z0 = spread(0, s0)
    sink_c.wait_recv()
    skz[z] = skc[0] + skc[1]
    sink_z = [send(skz.at[z], skz.at[z], at_z(step)) for step in range(1, NZ)]
    arrived(k_first, k_second)
    s2 = multiply(2, xc)
    z1 = spread(1, s1)
    z2 = spread(2, s2)
    for copy in y_near + y_pass:
        copy.wait_recv()
    total = dxo[...]
    for k in range(3):
        total = total + yr[k].astype(F32)
    dx_out[...] = total.astype(BF)
    wo_out[...] = collect(0, z0).T
    wq_out[...] = collect(1, z1)
    for copy in sink_z:
        copy.wait_recv()
    total = skz[0]
    for k in range(1, NZ):
        total = total + skz[k]
    sink_out[...] = total
    last = collect(2, z2)
    wk_out[...] = last[:, :KC]
    wv_out[...] = last[:, KC:]
    for copy in started:
        copy.wait_send()


def per_device(
    layer_input, output_grad, query_weight, key_weight, value_weight, out_weight, sink_logit
):
    vmem = pltpu.VMEM
    anywhere = pl.BlockSpec(memory_space=pl.ANY)
    inside = pl.BlockSpec(memory_space=pltpu.VMEM)
    outs = pl.pallas_call(
        kernel,
        name="attention_backward",
        out_shape=(
            jax.ShapeDtypeStruct((TOK, 1024), BF),
            jax.ShapeDtypeStruct((64, QC), F32),
            jax.ShapeDtypeStruct((64, KC), F32),
            jax.ShapeDtypeStruct((64, KC), F32),
            jax.ShapeDtypeStruct((QC, 64), F32),
            jax.ShapeDtypeStruct((8, 128), F32),
        ),
        in_specs=[anywhere] * 6 + [pl.BlockSpec(memory_space=pltpu.SMEM)],
        out_specs=[inside] * 6,
        scratch_shapes=[
            vmem((NY, 2, 4, TOK, 128), BF),
            vmem((NY, 2, 4, TOK, 128), BF),
            vmem((NY, 2, NX, TOK, 128), BF),
            vmem((NY, 2, NX, TOK, 128), BF),
            vmem((NY, 2, TOK, 128), BF),
            vmem((NY, 2, TOK, 128), BF),
            vmem((4096, QC), BF),
            vmem((4096, KC), BF),
            vmem((4096, KC), BF),
            vmem((QC, 4096), BF),
            vmem((TOK, QC + 2 * KC), F32),
            vmem((TOK, QC), F32),
            vmem((BAND, 2 * KC), BF),
            vmem((TOK, QC), BF),
            vmem((TOK, QC), BF),
            vmem((2, 2 * TOK, BAND), F32),
            vmem((2, 2 * TOK, 1), F32),
            vmem((3, NX, TOK, QC), BF),
            vmem((BAND, 2 * KC), F32),
            vmem((2, WINDOW, 2 * KC), BF),
            vmem((2, WINDOW, 2 * KC), BF),
            vmem((3, NY, 2, NC, 64, QC), F32),
            vmem((3, NY, 2, NC, 64, QC), BF),
            vmem((3, NY, 2, 64, QC), BF),
            vmem((3, NY, 2, 64, QC), BF),
            vmem((3, NZ - 1, 64, QC), BF),
            vmem((3, TOK, 1024), BF),
            vmem((3, TOK, 1024), BF),
            vmem((2, TOK // 2, 1024), BF),
            vmem((TOK, 1024), F32),
            vmem((NX, 8, 128), F32),
            vmem((NC, 8, 128), F32),
            vmem((NZ, 8, 128), F32),
            pltpu.SemaphoreType.DMA((20,)),
            pltpu.SemaphoreType.DMA((COPIES,)),
            pltpu.SemaphoreType.DMA((COPIES,)),
        ],
        compiler_params=pltpu.CompilerParams(
            collective_id=0, has_side_effects=True, vmem_limit_bytes=60 * 1024 * 1024
        ),
    )(layer_input, output_grad, query_weight, key_weight, value_weight, out_weight, sink_logit)
    return outs[:5] + (outs[5][0, :4],)


def solution(mesh):
    placed = (
        P("sp", "tp"),
        P("sp", "tp"),
        P(None, "tp"),
        P(None, "tp"),
        P(None, "tp"),
        P("tp", None),
        P("tp"),
    )
    return jax.shard_map(
        per_device,
        mesh=mesh,
        in_specs=placed,
        out_specs=(
            P("sp", "tp"),
            P("sp", "tp"),
            P("sp", "tp"),
            P("sp", "tp"),
            P("tp", "sp"),
            P("tp"),
        ),
        check_vma=False,
    )
```

```python
import jax
import jax.numpy as jnp
from jax import lax
from jax.experimental import pallas as pl
from jax.experimental.pallas import tpu as pltpu
from jax.sharding import PartitionSpec as P

HEAD = 128
WINDOW = 128
NZ, NX, NC, NY = 8, 4, 2, 4
TOK = 160
SEQ = TOK * NZ * NX * NC
BAND = TOK + 2 * WINDOW
QC = 512
KC = 256
SCALING = HEAD ** (-0.5)
MASKED = -1e30
BF = jnp.bfloat16
F32 = jnp.float32
COPIES = 160


def mm(left, right, left_dim, right_dim):
    return lax.dot_general(
        left, right, (((left_dim,), (right_dim,)), ((), ())), preferred_element_type=F32
    )


def kernel(
    x_hbm, g_hbm, wq_hbm, wk_hbm, wv_hbm, wo_hbm, sink_ref,
    dx_out, wq_out, wk_out, wv_out, wo_out, sink_out,
    xg, dg, xc, dc, wq, wk, wv, wo, acc, dacc, band, queries, grads,
    soft, psink, gc, kvg, hs, hr, pf, pb, sr, zs, zr, ys, yr, dxo, skx, skc, skz,
    local_sem, send_sem, recv_sem,
):
    sp = lax.axis_index("sp")
    y = lax.axis_index("tp")
    z = sp // (NX * NC)
    x = lax.rem(sp // NC, NX)
    c = lax.rem(sp, NC)

    def at_y(step):
        return (sp, lax.rem(y + step, NY))

    def at_x(step):
        return ((z * NX + lax.rem(x + step, NX)) * NC + c, y)

    def at_z(step):
        return ((lax.rem(z + step, NZ) * NX + x) * NC + c, y)

    sister = (sp + 1 - 2 * c, y)
    after = (lax.rem(sp + 1, NZ * NX * NC), y)
    before = (lax.rem(sp + NZ * NX * NC - 1, NZ * NX * NC), y)
    up, down = at_y(1), at_y(3)
    right, left = at_x(1), at_x(3)

    started = []
    local_count = [0]

    def send(src, dst, device):
        k = len(started)
        copy = pltpu.make_async_remote_copy(
            src_ref=src,
            dst_ref=dst,
            send_sem=send_sem.at[k],
            recv_sem=recv_sem.at[k],
            device_id=device,
            device_id_type=pl.DeviceIdType.MESH,
        )
        copy.start()
        started.append(copy)
        return copy

    def load(src, dst):
        k = local_count[0]
        local_count[0] += 1
        copy = pltpu.make_async_copy(src, dst, local_sem.at[k])
        copy.start()
        return copy

    def loads(hbm, blocks):
        return [
            load(hbm.at[:, pl.ds(k * 128, 128)], blocks.at[0, k // 4, k % 4]) for k in range(8)
        ]

    x_loads = loads(x_hbm, xg)
    d_loads = loads(g_hbm, dg)
    weight_loads = [load(wq_hbm, wq), load(wk_hbm, wk), load(wv_hbm, wv)]
    out_load = load(wo_hbm, wo)

    barrier = pltpu.get_barrier_semaphore()
    peers = [up, down, at_y(2), right, left, at_x(2), sister, after, before, at_z(1), at_z(7)]
    for peer in peers:
        pl.semaphore_signal(
            barrier, inc=1, device_id=peer, device_id_type=pl.DeviceIdType.MESH
        )
    pl.semaphore_wait(barrier, len(peers))

    class Gather:
        def __init__(self, piece, count, plus, minus):
            self.piece, self.count, self.plus, self.minus = piece, count, plus, minus
            self.ahead, self.behind, self.far = {}, {}, []
            for i in range(count):
                k = count - 1 - i
                self.ahead[i] = send(piece(0, i), piece(1, i), plus)
                self.behind[k] = send(piece(0, k), piece(3, k), minus)

        def forward(self):
            for i in range(self.count // 2):
                k = self.count - 1 - i
                self.ahead[i].wait_recv()
                self.far.append(send(self.piece(1, i), self.piece(2, i), self.plus))
                self.behind[k].wait_recv()
                self.far.append(send(self.piece(3, k), self.piece(2, k), self.minus))

        def wait_near(self):
            for i in range(self.count // 2, self.count):
                self.ahead[i].wait_recv()
                self.behind[self.count - 1 - i].wait_recv()

        def wait_far(self):
            for copy in self.far:
                copy.wait_recv()

    def quarters(blocks):
        return lambda ry, i: blocks.at[ry, i // 2, pl.ds(2 * (i % 2), 2)]

    def exchange(blocks, cells, ry):
        copies = [
            send(blocks.at[ry, :, lax.rem(x + step, NX)], cells.at[ry, :, step], at_x(step))
            for step in (2, 1, 3)
        ]
        for h in range(2):
            cells[ry, h, 0] = blocks[ry, h, x]
        return copies

    def wide(blocks, ry):
        return jnp.concatenate([blocks[ry, h, k] for h in range(2) for k in range(4)], axis=1)

    def features(ry):
        return pl.multiple_of(lax.rem(y + NY - ry, NY) * 1024, 1024)

    def project(ry):
        rows = pl.ds(features(ry), 1024)
        block = wide(xg, ry)
        for cols, weight in (
            (slice(0, QC), wq),
            (slice(QC, QC + KC), wk),
            (slice(QC + KC, QC + 2 * KC), wv),
        ):
            term = mm(block, weight[rows, :], 1, 0)
            acc[:, cols] = term if ry == 0 else acc[:, cols] + term

    def project_grad(ry):
        cols = pl.ds(features(ry), 1024)
        term = mm(wide(dg, ry), wo[:, cols], 1, 1)
        dacc[...] = term if ry == 0 else dacc[...] + term

    for copy in x_loads:
        copy.wait()
    x_gather = Gather(quarters(xg), 4, up, down)
    x_cells = exchange(xg, xc, 0)
    for copy in d_loads:
        copy.wait()
    d_cells = exchange(dg, dc, 0)
    for copy in weight_loads:
        copy.wait()
    project(0)
    x_gather.forward()
    d_gather = Gather(quarters(dg), 4, up, down)
    x_gather.wait_near()
    x_cells += exchange(xg, xc, 1)
    x_cells += exchange(xg, xc, 3)
    project(1)
    project(3)
    x_gather.wait_far()
    x_cells += exchange(xg, xc, 2)
    project(2)

    band[WINDOW : WINDOW + TOK, :] = acc[:, QC : QC + 2 * KC].astype(BF)
    queries[...] = acc[:, :QC].astype(BF)
    halo_after = send(band.at[pl.ds(TOK, WINDOW)], band.at[pl.ds(0, WINDOW)], after)
    halo_before = send(
        band.at[pl.ds(WINDOW, WINDOW)], band.at[pl.ds(WINDOW + TOK, WINDOW)], before
    )
    d_gather.forward()
    for copy in d_cells:
        copy.wait_recv()
    dc_gather = Gather(lambda ry, h: dc.at[ry, h, pl.ds(1, 3)], 2, up, down)
    out_load.wait()
    project_grad(0)
    halo_after.wait_recv()
    halo_before.wait_recv()

    row = lax.broadcasted_iota(jnp.int32, (2 * TOK, BAND), 0)
    row = jnp.where(row >= TOK, row - TOK, row)
    col = lax.broadcasted_iota(jnp.int32, (2 * TOK, BAND), 1) - WINDOW
    key_pos = sp * TOK + col
    in_window = (jnp.abs(row - col) <= WINDOW) & (key_pos >= 0) & (key_pos < SEQ)
    second_head = lax.broadcasted_iota(jnp.int32, (2 * TOK, 1), 0) >= TOK

    def heads(ref, kh):
        cols = kh * 2 * HEAD
        return jnp.concatenate(
            [ref[:, cols : cols + HEAD], ref[:, cols + HEAD : cols + 2 * HEAD]], axis=0
        )

    def put_heads(group, kh, value):
        gc[group, 2 * kh, 0] = value[:TOK].astype(BF)
        gc[group, 2 * kh + 1, 0] = value[TOK:].astype(BF)

    for kh in range(2):
        keys = band[:, kh * HEAD : (kh + 1) * HEAD]
        values = band[:, KC + kh * HEAD : KC + (kh + 1) * HEAD]
        scores = mm(heads(queries, kh), keys, 1, 1) * SCALING
        scores = jnp.where(in_window, scores, MASKED)
        sink = jnp.where(second_head, sink_ref[2 * kh + 1], sink_ref[2 * kh])
        row_max = jnp.maximum(jnp.max(scores, axis=1, keepdims=True), sink)
        weights = jnp.exp(scores - row_max)
        sink_weight = jnp.exp(sink - row_max)
        inverse = 1.0 / (jnp.sum(weights, axis=1, keepdims=True) + sink_weight)
        weights = weights * inverse
        soft[kh] = weights
        psink[kh] = sink_weight * inverse
        put_heads(0, kh, mm(weights.astype(BF), values, 1, 0))

    def share(group):
        return Gather(lambda r, i: gc.at[group, i, r], 4, right, left)

    shares = {0: share(0)}
    d_gather.wait_near()
    for ry in (1, 3):
        project_grad(ry)
        for h in range(2):
            dc[ry, h, 0] = dg[ry, h, x]
    d_gather.wait_far()
    project_grad(2)
    for h in range(2):
        dc[2, h, 0] = dg[2, h, x]
    grads[...] = dacc[...].astype(BF)

    lane = lax.broadcasted_iota(jnp.int32, (8, 128), 1)
    sink_tile = jnp.zeros((8, 128), F32)
    for kh in range(2):
        keys = band[:, kh * HEAD : (kh + 1) * HEAD]
        values = band[:, KC + kh * HEAD : KC + (kh + 1) * HEAD]
        query = heads(queries, kh)
        grad = heads(grads, kh)
        attended = jnp.concatenate([gc[0, 2 * kh, 0], gc[0, 2 * kh + 1, 0]], axis=0)
        row_dots = jnp.sum(grad.astype(F32) * attended.astype(F32), axis=1, keepdims=True)
        weights = soft[kh]
        prob_grads = mm(grad, values, 1, 1)
        score_grads = (weights * (prob_grads - row_dots)).astype(BF)
        put_heads(1, kh, mm(score_grads, keys, 1, 0) * SCALING)
        kvg[:, kh * HEAD : (kh + 1) * HEAD] = mm(score_grads, query, 0, 0) * SCALING
        kvg[:, KC + kh * HEAD : KC + (kh + 1) * HEAD] = mm(weights.astype(BF), grad, 0, 0)
        sink_rows = psink[kh] * row_dots
        for g in range(2):
            total = -jnp.sum(sink_rows[g * TOK : (g + 1) * TOK], axis=0, keepdims=True)
            sink_tile = jnp.where(lane == 2 * kh + g, total, sink_tile)
    hs[0] = kvg[0:WINDOW, :].astype(BF)
    hs[1] = kvg[WINDOW + TOK : BAND, :].astype(BF)
    back = send(hs.at[0], hr.at[0], before)
    forth = send(hs.at[1], hr.at[1], after)
    shares[1] = share(1)
    skx[x] = sink_tile
    sink_x = [send(skx.at[x], skx.at[x], at_x(step)) for step in (1, 3, 2)]

    dc_gather.forward()
    shares[0].forward()
    back.wait_recv()
    forth.wait_recv()
    kvg[TOK : WINDOW + TOK, :] += hr[0].astype(F32)
    kvg[WINDOW : 2 * WINDOW, :] += hr[1].astype(F32)
    for k in range(4):
        gc[2, k, 0] = kvg[WINDOW : WINDOW + TOK, k * HEAD : (k + 1) * HEAD].astype(BF)
    shares[2] = share(2)

    def input_share(step):
        rows = pl.ds(pl.multiple_of(lax.rem(y + step, NY) * 1024, 1024), 1024)
        own = [jnp.concatenate([gc[g, k, 0] for k in range(4)], axis=1) for g in (1, 2)]
        return (
            mm(own[0], wq[rows, :], 1, 1)
            + mm(own[1][:, :KC], wk[rows, :], 1, 1)
            + mm(own[1][:, KC:], wv[rows, :], 1, 1)
        )

    def input_send(step):
        ys[step - 1] = input_share(step).astype(BF)
        return send(ys.at[step - 1], yr.at[step - 1], at_y(step))

    y_copies = [input_send(2)]
    shares[1].forward()
    y_copies.append(input_send(1))
    y_copies.append(input_send(3))
    dc_gather.wait_near()
    dc_gather.wait_far()
    shares[0].wait_near()
    shares[0].wait_far()

    def multiply(group, cells):
        rows = jnp.concatenate(
            [cells[ry, h].reshape(NX * TOK, 128) for ry in range(NY) for h in range(2)], axis=1
        )
        cols = jnp.concatenate(
            [gc[group, k].reshape(NX * TOK, 128) for k in range(4)], axis=1
        )
        product = mm(rows, cols, 0, 0).reshape(NY, 2, NC, 64, QC)
        pf[group] = product
        pb[group] = product.astype(BF)
        return send(pb.at[group, :, :, 1 - c], sr.at[group], sister)

    class Ring:
        def __init__(self, group, from_sister, parts):
            self.group = group
            from_sister.wait_recv()
            width = QC // parts
            self.slices = [slice(p * width, (p + 1) * width) for p in range(parts)]
            self.copies = {}
            self.hop(0)

        def own(self, step, cols):
            to = lax.rem(z + step, NZ)
            ry = lax.rem(y + NY - to // 2, NY)
            h = lax.rem(to, 2)
            mine = pf[self.group, ry, h, c, :, cols]
            return mine + sr[self.group, ry, h, :, cols].astype(F32)

        def hop(self, k):
            for p, cols in enumerate(self.slices):
                for way, step in ((0, 4 - k), (1, 5 + k)):
                    if way == 1 and k == 3:
                        continue
                    total = self.own(step, cols)
                    if k > 0:
                        self.copies[way, k - 1, p].wait_recv()
                        total = total + zr[self.group, way, k - 1, :, cols].astype(F32)
                    zs[self.group, way, k, :, cols] = total.astype(BF)
                    span = pl.ds(cols.start, cols.stop - cols.start)
                    self.copies[way, k, p] = send(
                        zs.at[self.group, way, k, :, span],
                        zr.at[self.group, way, k, :, span],
                        at_z(1 if way == 0 else 7),
                    )

        def finish(self, p):
            cols = self.slices[p]
            total = self.own(0, cols)
            for way, k in ((1, 2), (0, 3)):
                self.copies[way, k, p].wait_recv()
                total = total + zr[self.group, way, k, :, cols].astype(F32)
            return total

    s0 = multiply(0, dc)
    for copy in sink_x:
        copy.wait_recv()
    skc[c] = (skx[0] + skx[1]) + (skx[2] + skx[3])
    sink_c = send(skc.at[c], skc.at[c], sister)
    shares[2].forward()
    ring0 = Ring(0, s0, 1)
    for copy in x_cells:
        copy.wait_recv()
    shares[1].wait_near()
    shares[1].wait_far()
    s1 = multiply(1, xc)
    ring0.hop(1)
    ring1 = Ring(1, s1, 1)
    shares[2].wait_near()
    shares[2].wait_far()
    s2 = multiply(2, xc)
    sink_c.wait_recv()
    skz[z] = skc[0] + skc[1]
    sink_z = []

    def sink_hop(k):
        for way, sign in ((0, -1), (1, 1)):
            if way == 1 and k == 3:
                continue
            if k > 0:
                sink_z[2 * (k - 1) + way].wait_recv()
            tile = skz.at[lax.rem(z + NZ + sign * k, NZ)]
            sink_z.append(send(tile, tile, at_z(1 if way == 0 else 7)))

    sink_hop(0)
    ring0.hop(2)
    ring1.hop(1)
    ring2 = Ring(2, s2, 2)
    ring0.hop(3)
    sink_hop(1)
    ring1.hop(2)
    ring2.hop(1)
    dxo[...] = input_share(0)
    sink_hop(2)
    ring1.hop(3)
    ring2.hop(2)
    wo_out[...] = ring0.finish(0)
    ring2.hop(3)
    sink_hop(3)
    for copy in y_copies:
        copy.wait_recv()
    total = dxo[...]
    for k in range(3):
        total = total + yr[k].astype(F32)
    dx_out[...] = total.astype(BF)
    wq_out[...] = ring1.finish(0)
    wk_out[...] = ring2.finish(0)
    wv_out[...] = ring2.finish(1)
    for copy in sink_z[5:]:
        copy.wait_recv()
    total = skz[0]
    for k in range(1, NZ):
        total = total + skz[k]
    sink_out[...] = total
    for copy in started:
        copy.wait_send()


def finish(*refs):
    for source, target in zip(refs[:5], refs[6:11]):
        target[...] = source[...]
    refs[11][...] = refs[5][0:1, 0:4]


def per_device(
    layer_input, output_grad, query_weight, key_weight, value_weight, out_weight, sink_logit
):
    vmem = pltpu.VMEM
    outside = pl.BlockSpec(memory_space=pltpu.HBM)
    inside = pl.BlockSpec(memory_space=pltpu.VMEM)
    results = (
        jax.ShapeDtypeStruct((TOK, 1024), BF),
        jax.ShapeDtypeStruct((64, QC), F32),
        jax.ShapeDtypeStruct((64, KC), F32),
        jax.ShapeDtypeStruct((64, KC), F32),
        jax.ShapeDtypeStruct((64, QC), F32),
    )
    outs = pl.pallas_call(
        kernel,
        name="attention_backward",
        out_shape=results + (jax.ShapeDtypeStruct((8, 128), F32),),
        in_specs=[outside] * 6 + [pl.BlockSpec(memory_space=pltpu.SMEM)],
        out_specs=[inside] * 6,
        scratch_shapes=[
            vmem((NY, 2, 4, TOK, 128), BF),
            vmem((NY, 2, 4, TOK, 128), BF),
            vmem((NY, 2, NX, TOK, 128), BF),
            vmem((NY, 2, NX, TOK, 128), BF),
            vmem((4096, QC), BF),
            vmem((4096, KC), BF),
            vmem((4096, KC), BF),
            vmem((QC, 4096), BF),
            vmem((TOK, QC + 2 * KC), F32),
            vmem((TOK, QC), F32),
            vmem((BAND, 2 * KC), BF),
            vmem((TOK, QC), BF),
            vmem((TOK, QC), BF),
            vmem((2, 2 * TOK, BAND), F32),
            vmem((2, 2 * TOK, 1), F32),
            vmem((3, 4, NX, TOK, 128), BF),
            vmem((BAND, 2 * KC), F32),
            vmem((2, WINDOW, 2 * KC), BF),
            vmem((2, WINDOW, 2 * KC), BF),
            vmem((3, NY, 2, NC, 64, QC), F32),
            vmem((3, NY, 2, NC, 64, QC), BF),
            vmem((3, NY, 2, 64, QC), BF),
            vmem((3, 2, 4, 64, QC), BF),
            vmem((3, 2, 4, 64, QC), BF),
            vmem((3, TOK, 1024), BF),
            vmem((3, TOK, 1024), BF),
            vmem((TOK, 1024), F32),
            vmem((NX, 8, 128), F32),
            vmem((NC, 8, 128), F32),
            vmem((NZ, 8, 128), F32),
            pltpu.SemaphoreType.DMA((20,)),
            pltpu.SemaphoreType.DMA((COPIES,)),
            pltpu.SemaphoreType.DMA((COPIES,)),
        ],
        compiler_params=pltpu.CompilerParams(
            collective_id=0, has_side_effects=True, vmem_limit_bytes=50 * 1024 * 1024
        ),
    )(layer_input, output_grad, query_weight, key_weight, value_weight, out_weight, sink_logit)
    outs = pl.pallas_call(
        finish,
        name="finish",
        out_shape=results + (jax.ShapeDtypeStruct((1, 4), F32),),
        in_specs=[inside] * 6,
        out_specs=[inside] * 6,
        compiler_params=pltpu.CompilerParams(vmem_limit_bytes=8 * 1024 * 1024),
    )(*outs)
    return outs[:4] + (outs[4].T, outs[5].reshape(4))


def solution(mesh):
    placed = (
        P("sp", "tp"),
        P("sp", "tp"),
        P(None, "tp"),
        P(None, "tp"),
        P(None, "tp"),
        P("tp", None),
        P("tp"),
    )
    return jax.shard_map(
        per_device,
        mesh=mesh,
        in_specs=placed,
        out_specs=(
            P("sp", "tp"),
            P("sp", "tp"),
            P("sp", "tp"),
            P("sp", "tp"),
            P("tp", "sp"),
            P("tp"),
        ),
        check_vma=False,
    )
```

```python
import jax
import jax.numpy as jnp
from jax import lax
from jax.experimental import pallas as pl
from jax.experimental.pallas import tpu as pltpu
from jax.sharding import PartitionSpec as P

HEAD = 128
WINDOW = 128
NZ, NX, NC, NY = 8, 4, 2, 4
TOK = 160
SEQ = TOK * NZ * NX * NC
BAND = TOK + 2 * WINDOW
QC = 512
KC = 256
SCALING = HEAD ** (-0.5)
MASKED = -1e30
BF = jnp.bfloat16
F32 = jnp.float32
COPIES = 176


def mm(left, right, left_dim, right_dim):
    return lax.dot_general(
        left, right, (((left_dim,), (right_dim,)), ((), ())), preferred_element_type=F32
    )


def kernel(
    x_hbm, g_hbm, wq_hbm, wk_hbm, wv_hbm, wo_hbm, sink_ref,
    dx_out, wq_out, wk_out, wv_out, wo_out, sink_out,
    xg, dg, xc, dc, xt, dt, wq, wk, wv, wo, acc, dacc, band, queries, grads,
    soft, psink, gc, kvg, hs, hr, pf, pb, sr, zs, zr, ys, yr, yrelay, dxo, skx, skc, skz,
    local_sem, send_sem, recv_sem,
):
    sp = lax.axis_index("sp")
    y = lax.axis_index("tp")
    z = sp // (NX * NC)
    x = lax.rem(sp // NC, NX)
    c = lax.rem(sp, NC)

    def at_y(step):
        return (sp, lax.rem(y + step, NY))

    def at_x(step):
        return ((z * NX + lax.rem(x + step, NX)) * NC + c, y)

    def at_z(step):
        return ((lax.rem(z + step, NZ) * NX + x) * NC + c, y)

    sister = (sp + 1 - 2 * c, y)
    after = (lax.rem(sp + 1, NZ * NX * NC), y)
    before = (lax.rem(sp + NZ * NX * NC - 1, NZ * NX * NC), y)
    up, down = at_y(1), at_y(3)
    right, left = at_x(1), at_x(3)

    started = []
    local_count = [0]

    def send(src, dst, device):
        k = len(started)
        copy = pltpu.make_async_remote_copy(
            src_ref=src,
            dst_ref=dst,
            send_sem=send_sem.at[k],
            recv_sem=recv_sem.at[k],
            device_id=device,
            device_id_type=pl.DeviceIdType.MESH,
        )
        copy.start()
        started.append(copy)
        return copy

    def load(src, dst):
        k = local_count[0]
        local_count[0] += 1
        copy = pltpu.make_async_copy(src, dst, local_sem.at[k])
        copy.start()
        return copy

    def loads(hbm, blocks):
        return [
            load(hbm.at[:, pl.ds(k * 128, 128)], blocks.at[0, k // 4, k % 4]) for k in range(8)
        ]

    x_loads = loads(x_hbm, xg)
    d_loads = loads(g_hbm, dg)
    weight_loads = [load(wq_hbm, wq), load(wk_hbm, wk), load(wv_hbm, wv)]
    out_load = load(wo_hbm, wo)

    barrier = pltpu.get_barrier_semaphore()
    peers = [up, down, at_y(2), right, left, at_x(2), sister, after, before, at_z(1), at_z(7)]
    for peer in peers:
        pl.semaphore_signal(
            barrier, inc=1, device_id=peer, device_id_type=pl.DeviceIdType.MESH
        )
    pl.semaphore_wait(barrier, len(peers))

    class Gather:
        def __init__(self, piece, count, plus, minus):
            self.piece, self.count, self.plus, self.minus = piece, count, plus, minus
            self.ahead, self.behind, self.far = {}, {}, []
            for i in range(count):
                k = count - 1 - i
                self.ahead[i] = send(piece(0, i), piece(1, i), plus)
                self.behind[k] = send(piece(0, k), piece(3, k), minus)

        def forward(self):
            for i in range(self.count // 2):
                k = self.count - 1 - i
                self.ahead[i].wait_recv()
                self.far.append(send(self.piece(1, i), self.piece(2, i), self.plus))
                self.behind[k].wait_recv()
                self.far.append(send(self.piece(3, k), self.piece(2, k), self.minus))

        def wait_near(self):
            for i in range(self.count // 2, self.count):
                self.ahead[i].wait_recv()
                self.behind[self.count - 1 - i].wait_recv()

        def wait_far(self):
            for copy in self.far:
                copy.wait_recv()

    def quarters(blocks):
        return lambda ry, i: blocks.at[ry, i // 2, pl.ds(2 * (i % 2), 2)]

    def exchange(blocks, cells, ry):
        which = pl.ds(0, 2) if ry == 0 else 1
        copies = [
            send(blocks.at[ry, which, lax.rem(x + step, NX)], cells.at[ry, which, step], at_x(step))
            for step in (2, 1, 3)
        ]
        for h in range(2):
            cells[ry, h, 0] = blocks[ry, h, x]
        return copies

    def wide(blocks, ry):
        return jnp.concatenate([blocks[ry, h, k] for h in range(2) for k in range(4)], axis=1)

    def features(ry):
        return pl.multiple_of(lax.rem(y + NY - ry, NY) * 1024, 1024)

    def project(ry):
        rows = pl.ds(features(ry), 1024)
        block = wide(xg, ry)
        for cols, weight in (
            (slice(0, QC), wq),
            (slice(QC, QC + KC), wk),
            (slice(QC + KC, QC + 2 * KC), wv),
        ):
            term = mm(block, weight[rows, :], 1, 0)
            acc[:, cols] = term if ry == 0 else acc[:, cols] + term

    def project_grad(ry):
        cols = pl.ds(features(ry), 1024)
        term = mm(wide(dg, ry), wo[:, cols], 1, 1)
        dacc[...] = term if ry == 0 else dacc[...] + term

    for copy in x_loads:
        copy.wait()
    x_gather = Gather(quarters(xg), 4, up, down)
    x_cells = exchange(xg, xc, 0)
    for copy in d_loads:
        copy.wait()
    d_cells = exchange(dg, dc, 0)
    for copy in weight_loads:
        copy.wait()
    project(0)
    x_gather.forward()
    d_gather = Gather(quarters(dg), 4, up, down)
    x_gather.wait_near()
    x_cells += exchange(xg, xc, 1)
    x_cells += exchange(xg, xc, 3)
    project(1)
    project(3)
    x_gather.wait_far()
    project(2)

    band[WINDOW : WINDOW + TOK, :] = acc[:, QC : QC + 2 * KC].astype(BF)
    queries[...] = acc[:, :QC].astype(BF)
    halo_after = send(band.at[pl.ds(TOK, WINDOW)], band.at[pl.ds(0, WINDOW)], after)
    halo_before = send(
        band.at[pl.ds(WINDOW, WINDOW)], band.at[pl.ds(WINDOW + TOK, WINDOW)], before
    )
    x_cells += exchange(xg, xc, 2)
    d_gather.forward()
    for copy in d_cells:
        copy.wait_recv()
    dc_gather = Gather(lambda ry, h: dc.at[ry, h, pl.ds(1, 3)], 2, up, down)
    out_load.wait()
    project_grad(0)
    halo_after.wait_recv()
    halo_before.wait_recv()

    row = lax.broadcasted_iota(jnp.int32, (2 * TOK, BAND), 0)
    row = jnp.where(row >= TOK, row - TOK, row)
    col = lax.broadcasted_iota(jnp.int32, (2 * TOK, BAND), 1) - WINDOW
    key_pos = sp * TOK + col
    in_window = (jnp.abs(row - col) <= WINDOW) & (key_pos >= 0) & (key_pos < SEQ)
    second_head = lax.broadcasted_iota(jnp.int32, (2 * TOK, 1), 0) >= TOK

    def heads(ref, kh):
        cols = kh * 2 * HEAD
        return jnp.concatenate(
            [ref[:, cols : cols + HEAD], ref[:, cols + HEAD : cols + 2 * HEAD]], axis=0
        )

    def put_heads(group, kh, value):
        gc[group, 2 * kh, 0] = value[:TOK].astype(BF)
        gc[group, 2 * kh + 1, 0] = value[TOK:].astype(BF)

    for kh in range(2):
        keys = band[:, kh * HEAD : (kh + 1) * HEAD]
        values = band[:, KC + kh * HEAD : KC + (kh + 1) * HEAD]
        scores = mm(heads(queries, kh), keys, 1, 1) * SCALING
        scores = jnp.where(in_window, scores, MASKED)
        sink = jnp.where(second_head, sink_ref[2 * kh + 1], sink_ref[2 * kh])
        row_max = jnp.maximum(jnp.max(scores, axis=1, keepdims=True), sink)
        weights = jnp.exp(scores - row_max)
        sink_weight = jnp.exp(sink - row_max)
        inverse = 1.0 / (jnp.sum(weights, axis=1, keepdims=True) + sink_weight)
        weights = weights * inverse
        soft[kh] = weights
        psink[kh] = sink_weight * inverse
        put_heads(0, kh, mm(weights.astype(BF), values, 1, 0))

    def share(group):
        return Gather(lambda r, i: gc.at[group, i, r], 4, right, left)

    shares = {0: share(0)}
    d_gather.wait_near()
    for ry in (1, 3):
        project_grad(ry)
        for h in range(2):
            dc[ry, h, 0] = dg[ry, h, x]
    d_gather.wait_far()
    project_grad(2)
    for h in range(2):
        dc[2, h, 0] = dg[2, h, x]
    grads[...] = dacc[...].astype(BF)

    shares[0].forward()
    lane = lax.broadcasted_iota(jnp.int32, (8, 128), 1)
    sink_tile = jnp.zeros((8, 128), F32)
    for kh in range(2):
        keys = band[:, kh * HEAD : (kh + 1) * HEAD]
        values = band[:, KC + kh * HEAD : KC + (kh + 1) * HEAD]
        query = heads(queries, kh)
        grad = heads(grads, kh)
        attended = jnp.concatenate([gc[0, 2 * kh, 0], gc[0, 2 * kh + 1, 0]], axis=0)
        row_dots = jnp.sum(grad.astype(F32) * attended.astype(F32), axis=1, keepdims=True)
        weights = soft[kh]
        prob_grads = mm(grad, values, 1, 1)
        score_grads = (weights * (prob_grads - row_dots)).astype(BF)
        put_heads(1, kh, mm(score_grads, keys, 1, 0) * SCALING)
        kvg[:, kh * HEAD : (kh + 1) * HEAD] = mm(score_grads, query, 0, 0) * SCALING
        kvg[:, KC + kh * HEAD : KC + (kh + 1) * HEAD] = mm(weights.astype(BF), grad, 0, 0)
        sink_rows = psink[kh] * row_dots
        for g in range(2):
            total = -jnp.sum(sink_rows[g * TOK : (g + 1) * TOK], axis=0, keepdims=True)
            sink_tile = jnp.where(lane == 2 * kh + g, total, sink_tile)
    hs[0] = kvg[0:WINDOW, :].astype(BF)
    hs[1] = kvg[WINDOW + TOK : BAND, :].astype(BF)
    back = send(hs.at[0], hr.at[0], before)
    forth = send(hs.at[1], hr.at[1], after)
    skx[x] = sink_tile

    def owner(step):
        return pl.ds(pl.multiple_of(lax.rem(y + step, NY) * 1024, 1024), 1024)

    def own_grads(group):
        return jnp.concatenate([gc[group, k, 0] for k in range(4)], axis=1)

    def input_share(step):
        own = own_grads(2)
        return (
            dxo[step]
            + mm(own[:, :KC], wk[owner(step), :], 1, 1)
            + mm(own[:, KC:], wv[owner(step), :], 1, 1)
        )

    low, high = pl.ds(0, TOK // 2), pl.ds(TOK // 2, TOK // 2)

    def input_far():
        ys[1] = input_share(2).astype(BF)
        return [
            send(ys.at[1, low], yrelay.at[0], up),
            send(ys.at[1, high], yrelay.at[1], down),
        ]

    def input_near(step, block, rows, device):
        dxo[step] = input_share(step)
        ys[block, rows, :] = dxo[step, rows, :].astype(BF)
        return send(ys.at[block, rows], yr.at[block // 2, rows], device)

    def input_pass(copies):
        for k, step, block, rows, device in ((0, 1, 0, low, up), (1, 3, 2, high, down)):
            copies[k].wait_recv()
            ys[block, rows, :] = (dxo[step, rows, :] + yrelay[k].astype(F32)).astype(BF)
            copies.append(send(ys.at[block, rows], yr.at[block // 2, rows], device))

    shares[1] = share(1)
    sink_x = [send(skx.at[x], skx.at[x], at_x(step)) for step in (1, 3, 2)]
    dc_gather.forward()
    for copy in x_cells:
        copy.wait_recv()
    xc_gather = Gather(
        lambda ry, i: xc.at[ry, 0, pl.ds(1, 3), pl.ds(i * (TOK // 2), TOK // 2)], 2, up, down
    )
    for step in (2, 1, 3, 0):
        dxo[step] = mm(own_grads(1), wq[owner(step), :], 1, 1)
    shares[1].forward()
    back.wait_recv()
    forth.wait_recv()
    kvg[TOK : WINDOW + TOK, :] += hr[0].astype(F32)
    kvg[WINDOW : 2 * WINDOW, :] += hr[1].astype(F32)
    for k in range(4):
        gc[2, k, 0] = kvg[WINDOW : WINDOW + TOK, k * HEAD : (k + 1) * HEAD].astype(BF)
    shares[2] = share(2)
    dc_gather.wait_near()
    dc_gather.wait_far()
    shares[0].wait_near()
    shares[0].wait_far()

    def turn(cells, turned, h):
        for ry in range(NY):
            turned[ry, h] = cells[ry, h].reshape(NX * TOK, 128).T

    def multiply(group, turned):
        cols = jnp.concatenate([gc[group, k].reshape(NX * TOK, 128) for k in range(4)], axis=1)

        def product(core):
            rows = pl.ds(pl.multiple_of(core * 64, 64), 64)
            left = jnp.concatenate(
                [turned[ry, h, rows, :] for ry in range(NY) for h in range(2)], axis=0
            )
            return mm(left, cols, 1, 0).reshape(NY, 2, 64, QC)

        pb[group] = product(1 - c).astype(BF)
        copy = send(pb.at[group], sr.at[group], sister)
        pf[group] = product(c)
        return copy

    class Ring:
        def __init__(self, group, from_sister, parts):
            self.group = group
            from_sister.wait_recv()
            width = QC // parts
            self.slices = [slice(p * width, (p + 1) * width) for p in range(parts)]
            self.copies = {}
            self.hop(0)

        def own(self, step, cols):
            to = lax.rem(z + step, NZ)
            ry = lax.rem(y + NY - to // 2, NY)
            h = lax.rem(to, 2)
            mine = pf[self.group, ry, h, :, cols]
            return mine + sr[self.group, ry, h, :, cols].astype(F32)

        def hop(self, k):
            for p, cols in enumerate(self.slices):
                for way, step in ((0, 4 - k), (1, 5 + k)):
                    if way == 1 and k == 3:
                        continue
                    toward = 1 if way == 0 else 7
                    if p % 2 == 1:
                        step, toward = NZ - step, NZ - toward
                    total = self.own(step, cols)
                    if k > 0:
                        self.copies[way, k - 1, p].wait_recv()
                        total = total + zr[self.group, way, k - 1, :, cols].astype(F32)
                    zs[self.group, way, k, :, cols] = total.astype(BF)
                    span = pl.ds(cols.start, cols.stop - cols.start)
                    self.copies[way, k, p] = send(
                        zs.at[self.group, way, k, :, span],
                        zr.at[self.group, way, k, :, span],
                        at_z(toward),
                    )

        def finish(self, p):
            cols = self.slices[p]
            total = self.own(0, cols)
            for way, k in ((1, 2), (0, 3)):
                self.copies[way, k, p].wait_recv()
                total = total + zr[self.group, way, k, :, cols].astype(F32)
            return total

    xc_gather.forward()
    turn(dc, dt, 0)
    turn(dc, dt, 1)
    s0 = multiply(0, dt)
    for copy in sink_x:
        copy.wait_recv()
    skc[c] = (skx[0] + skx[1]) + (skx[2] + skx[3])
    sink_c = send(skc.at[c], skc.at[c], sister)
    turn(xc, xt, 1)
    ring0 = Ring(0, s0, 2)
    xc_gather.wait_near()
    xc_gather.wait_far()
    turn(xc, xt, 0)
    shares[1].wait_near()
    shares[1].wait_far()
    shares[2].forward()
    s1 = multiply(1, xt)
    y_copies = input_far()
    ring0.hop(1)
    ring1 = Ring(1, s1, 2)
    y_copies.append(input_near(1, 0, high, up))
    shares[2].wait_near()
    shares[2].wait_far()
    s2 = multiply(2, xt)
    sink_c.wait_recv()
    skz[z] = skc[0] + skc[1]
    sink_z = []

    def sink_hop(k):
        for way, sign in ((0, -1), (1, 1)):
            if way == 1 and k == 3:
                continue
            if k > 0:
                sink_z[2 * (k - 1) + way].wait_recv()
            tile = skz.at[lax.rem(z + NZ + sign * k, NZ)]
            sink_z.append(send(tile, tile, at_z(1 if way == 0 else 7)))

    sink_hop(0)
    ring0.hop(2)
    ring1.hop(1)
    ring2 = Ring(2, s2, 4)
    y_copies.append(input_near(3, 2, low, down))
    sink_hop(1)
    ring0.hop(3)
    ring1.hop(2)
    ring2.hop(1)
    input_pass(y_copies)
    dxo[0] = input_share(0)
    sink_hop(2)
    ring1.hop(3)
    ring2.hop(2)
    sink_hop(3)
    for p, cols in enumerate(ring0.slices):
        wo_out[:, cols] = ring0.finish(p)
    ring2.hop(3)
    for copy in y_copies[2:]:
        copy.wait_recv()
    total = dxo[0]
    for k in range(2):
        total = total + yr[k].astype(F32)
    dx_out[...] = total.astype(BF)
    for p, cols in enumerate(ring1.slices):
        wq_out[:, cols] = ring1.finish(p)
    for copy in sink_z[5:]:
        copy.wait_recv()
    total = skz[0]
    for k in range(1, NZ):
        total = total + skz[k]
    sink_out[...] = total
    for p in range(2):
        wk_out[:, ring2.slices[p]] = ring2.finish(p)
        wv_out[:, ring2.slices[p]] = ring2.finish(p + 2)
    for copy in started:
        copy.wait_send()


def finish(*refs):
    for source, target in zip(refs[:5], refs[6:11]):
        target[...] = source[...]
    refs[11][...] = refs[5][0:1, 0:4]


def per_device(
    layer_input, output_grad, query_weight, key_weight, value_weight, out_weight, sink_logit
):
    vmem = pltpu.VMEM
    outside = pl.BlockSpec(memory_space=pltpu.HBM)
    inside = pl.BlockSpec(memory_space=pltpu.VMEM)
    results = (
        jax.ShapeDtypeStruct((TOK, 1024), BF),
        jax.ShapeDtypeStruct((64, QC), F32),
        jax.ShapeDtypeStruct((64, KC), F32),
        jax.ShapeDtypeStruct((64, KC), F32),
        jax.ShapeDtypeStruct((64, QC), F32),
    )
    outs = pl.pallas_call(
        kernel,
        name="attention_backward",
        out_shape=results + (jax.ShapeDtypeStruct((8, 128), F32),),
        in_specs=[outside] * 6 + [pl.BlockSpec(memory_space=pltpu.SMEM)],
        out_specs=[inside] * 6,
        scratch_shapes=[
            vmem((NY, 2, 4, TOK, 128), BF),
            vmem((NY, 2, 4, TOK, 128), BF),
            vmem((NY, 2, NX, TOK, 128), BF),
            vmem((NY, 2, NX, TOK, 128), BF),
        vmem((NY, 2, 128, NX * TOK), BF),
        vmem((NY, 2, 128, NX * TOK), BF),
            vmem((4096, QC), BF),
            vmem((4096, KC), BF),
            vmem((4096, KC), BF),
            vmem((QC, 4096), BF),
            vmem((TOK, QC + 2 * KC), F32),
            vmem((TOK, QC), F32),
            vmem((BAND, 2 * KC), BF),
            vmem((TOK, QC), BF),
            vmem((TOK, QC), BF),
            vmem((2, 2 * TOK, BAND), F32),
            vmem((2, 2 * TOK, 1), F32),
            vmem((3, 4, NX, TOK, 128), BF),
            vmem((BAND, 2 * KC), F32),
            vmem((2, WINDOW, 2 * KC), BF),
            vmem((2, WINDOW, 2 * KC), BF),
            vmem((3, NY, 2, 64, QC), F32),
            vmem((3, NY, 2, 64, QC), BF),
            vmem((3, NY, 2, 64, QC), BF),
            vmem((3, 2, 4, 64, QC), BF),
            vmem((3, 2, 4, 64, QC), BF),
            vmem((3, TOK, 1024), BF),
            vmem((2, TOK, 1024), BF),
        vmem((2, TOK // 2, 1024), BF),
            vmem((NY, TOK, 1024), F32),
            vmem((NX, 8, 128), F32),
            vmem((NC, 8, 128), F32),
            vmem((NZ, 8, 128), F32),
            pltpu.SemaphoreType.DMA((20,)),
            pltpu.SemaphoreType.DMA((COPIES,)),
            pltpu.SemaphoreType.DMA((COPIES,)),
        ],
        compiler_params=pltpu.CompilerParams(
            collective_id=0, has_side_effects=True, vmem_limit_bytes=53 * 1024 * 1024
        ),
    )(layer_input, output_grad, query_weight, key_weight, value_weight, out_weight, sink_logit)
    outs = pl.pallas_call(
        finish,
        name="finish",
        out_shape=results + (jax.ShapeDtypeStruct((1, 4), F32),),
        in_specs=[inside] * 6,
        out_specs=[inside] * 6,
        compiler_params=pltpu.CompilerParams(vmem_limit_bytes=8 * 1024 * 1024),
    )(*outs)
    return outs[:4] + (outs[4].T, outs[5].reshape(4))


def solution(mesh):
    placed = (
        P("sp", "tp"),
        P("sp", "tp"),
        P(None, "tp"),
        P(None, "tp"),
        P(None, "tp"),
        P("tp", None),
        P("tp"),
    )
    return jax.shard_map(
        per_device,
        mesh=mesh,
        in_specs=placed,
        out_specs=(
            P("sp", "tp"),
            P("sp", "tp"),
            P("sp", "tp"),
            P("sp", "tp"),
            P("tp", "sp"),
            P("tp"),
        ),
        check_vma=False,
    )
```

```python
import jax
import jax.numpy as jnp
from jax import lax
from jax.experimental import pallas as pl
from jax.experimental.pallas import tpu as pltpu
from jax.sharding import PartitionSpec as P

HEAD = 128
WINDOW = 128
NZ, NX, NC, NY = 8, 4, 2, 4
TOK = 160
SEQ = TOK * NZ * NX * NC
BAND = TOK + 2 * WINDOW
QC = 512
KC = 256
SCALING = HEAD ** (-0.5)
MASKED = -1e30
BF = jnp.bfloat16
F32 = jnp.float32
COPIES = 176


def mm(left, right, left_dim, right_dim):
    return lax.dot_general(
        left, right, (((left_dim,), (right_dim,)), ((), ())), preferred_element_type=F32
    )


def kernel(
    x_hbm, g_hbm, wq_hbm, wk_hbm, wv_hbm, wo_hbm, sink_ref,
    dx_out, wq_out, wk_out, wv_out, wo_out, sink_out,
    xg, dg, xc, dc, xt, dt, wq, wk, wv, wo, acc, dacc, band, queries, grads,
    soft, psink, gc, kvg, hs, hr, pf, pb, sr, zs, zr, ys, yr, yrelay, dxo, skx, skc, skz,
    local_sem, send_sem, recv_sem,
):
    sp = lax.axis_index("sp")
    y = lax.axis_index("tp")
    z = sp // (NX * NC)
    x = lax.rem(sp // NC, NX)
    c = lax.rem(sp, NC)

    def at_y(step):
        return (sp, lax.rem(y + step, NY))

    def at_x(step):
        return ((z * NX + lax.rem(x + step, NX)) * NC + c, y)

    def at_z(step):
        return ((lax.rem(z + step, NZ) * NX + x) * NC + c, y)

    sister = (sp + 1 - 2 * c, y)
    after = (lax.rem(sp + 1, NZ * NX * NC), y)
    before = (lax.rem(sp + NZ * NX * NC - 1, NZ * NX * NC), y)
    up, down = at_y(1), at_y(3)
    right, left = at_x(1), at_x(3)

    started = []
    local_count = [0]

    def send(src, dst, device):
        k = len(started)
        copy = pltpu.make_async_remote_copy(
            src_ref=src,
            dst_ref=dst,
            send_sem=send_sem.at[k],
            recv_sem=recv_sem.at[k],
            device_id=device,
            device_id_type=pl.DeviceIdType.MESH,
        )
        copy.start()
        started.append(copy)
        return copy

    def load(src, dst):
        k = local_count[0]
        local_count[0] += 1
        copy = pltpu.make_async_copy(src, dst, local_sem.at[k])
        copy.start()
        return copy

    def loads(hbm, blocks):
        return [
            load(hbm.at[:, pl.ds(k * 128, 128)], blocks.at[0, k // 4, k % 4]) for k in range(8)
        ]

    x_loads = loads(x_hbm, xg)
    d_loads = loads(g_hbm, dg)
    weight_loads = [load(wq_hbm, wq), load(wk_hbm, wk), load(wv_hbm, wv)]
    out_load = load(wo_hbm, wo)

    barrier = pltpu.get_barrier_semaphore()
    peers = [up, down, right, left, at_x(2), sister, after, before, at_z(1), at_z(7)]
    for peer in peers:
        pl.semaphore_signal(
            barrier, inc=1, device_id=peer, device_id_type=pl.DeviceIdType.MESH
        )
    pl.semaphore_wait(barrier, len(peers))

    class Gather:
        def __init__(self, piece, count, plus, minus):
            self.piece, self.count, self.plus, self.minus = piece, count, plus, minus
            self.ahead, self.behind, self.far = {}, {}, []
            for i in range(count):
                k = count - 1 - i
                self.ahead[i] = send(piece(0, i), piece(1, i), plus)
                self.behind[k] = send(piece(0, k), piece(3, k), minus)

        def forward(self):
            for i in range(self.count // 2):
                k = self.count - 1 - i
                self.ahead[i].wait_recv()
                self.far.append(send(self.piece(1, i), self.piece(2, i), self.plus))
                self.behind[k].wait_recv()
                self.far.append(send(self.piece(3, k), self.piece(2, k), self.minus))

        def wait_near(self):
            for i in range(self.count // 2, self.count):
                self.ahead[i].wait_recv()
                self.behind[self.count - 1 - i].wait_recv()

        def wait_far(self):
            for copy in self.far:
                copy.wait_recv()

    def quarters(blocks):
        return lambda ry, i: blocks.at[ry, i // 2, pl.ds(2 * (i % 2), 2)]

    def exchange(blocks, cells, ry):
        which = pl.ds(0, 2) if ry == 0 else 1
        copies = [
            send(blocks.at[ry, which, lax.rem(x + step, NX)], cells.at[ry, which, step], at_x(step))
            for step in (2, 1, 3)
        ]
        for h in range(2):
            cells[ry, h, 0] = blocks[ry, h, x]
        return copies

    def wide(blocks, ry):
        return jnp.concatenate([blocks[ry, h, k] for h in range(2) for k in range(4)], axis=1)

    def features(ry):
        return pl.multiple_of(lax.rem(y + NY - ry, NY) * 1024, 1024)

    def project(ry):
        rows = pl.ds(features(ry), 1024)
        block = wide(xg, ry)
        for cols, weight in (
            (slice(0, QC), wq),
            (slice(QC, QC + KC), wk),
            (slice(QC + KC, QC + 2 * KC), wv),
        ):
            term = mm(block, weight[rows, :], 1, 0)
            acc[:, cols] = term if ry == 0 else acc[:, cols] + term

    def project_grad(ry):
        cols = pl.ds(features(ry), 1024)
        term = mm(wide(dg, ry), wo[:, cols], 1, 1)
        dacc[...] = term if ry == 0 else dacc[...] + term

    for copy in x_loads:
        copy.wait()
    x_gather = Gather(quarters(xg), 4, up, down)
    x_cells = exchange(xg, xc, 0)
    for copy in d_loads:
        copy.wait()
    d_cells = exchange(dg, dc, 0)
    for copy in weight_loads:
        copy.wait()
    project(0)
    x_gather.forward()
    d_gather = Gather(quarters(dg), 4, up, down)
    x_gather.wait_near()
    x_cells += exchange(xg, xc, 1)
    x_cells += exchange(xg, xc, 3)
    project(1)
    project(3)
    x_gather.wait_far()
    project(2)

    band[WINDOW : WINDOW + TOK, :] = acc[:, QC : QC + 2 * KC].astype(BF)
    queries[...] = acc[:, :QC].astype(BF)
    halo_after = send(band.at[pl.ds(TOK, WINDOW)], band.at[pl.ds(0, WINDOW)], after)
    halo_before = send(
        band.at[pl.ds(WINDOW, WINDOW)], band.at[pl.ds(WINDOW + TOK, WINDOW)], before
    )
    x_cells += exchange(xg, xc, 2)
    d_gather.forward()
    for copy in d_cells:
        copy.wait_recv()
    dc_gather = Gather(lambda ry, h: dc.at[ry, h, pl.ds(1, 3)], 2, up, down)
    out_load.wait()
    project_grad(0)
    halo_after.wait_recv()
    halo_before.wait_recv()

    row = lax.broadcasted_iota(jnp.int32, (2 * TOK, BAND), 0)
    row = jnp.where(row >= TOK, row - TOK, row)
    col = lax.broadcasted_iota(jnp.int32, (2 * TOK, BAND), 1) - WINDOW
    key_pos = sp * TOK + col
    in_window = (jnp.abs(row - col) <= WINDOW) & (key_pos >= 0) & (key_pos < SEQ)
    second_head = lax.broadcasted_iota(jnp.int32, (2 * TOK, 1), 0) >= TOK

    def heads(ref, kh):
        cols = kh * 2 * HEAD
        return jnp.concatenate(
            [ref[:, cols : cols + HEAD], ref[:, cols + HEAD : cols + 2 * HEAD]], axis=0
        )

    def put_heads(group, kh, value):
        gc[group, 2 * kh, 0] = value[:TOK].astype(BF)
        gc[group, 2 * kh + 1, 0] = value[TOK:].astype(BF)

    for kh in range(2):
        keys = band[:, kh * HEAD : (kh + 1) * HEAD]
        values = band[:, KC + kh * HEAD : KC + (kh + 1) * HEAD]
        scores = mm(heads(queries, kh), keys, 1, 1) * SCALING
        scores = jnp.where(in_window, scores, MASKED)
        sink = jnp.where(second_head, sink_ref[2 * kh + 1], sink_ref[2 * kh])
        row_max = jnp.maximum(jnp.max(scores, axis=1, keepdims=True), sink)
        weights = jnp.exp(scores - row_max)
        sink_weight = jnp.exp(sink - row_max)
        inverse = 1.0 / (jnp.sum(weights, axis=1, keepdims=True) + sink_weight)
        weights = weights * inverse
        soft[kh] = weights
        psink[kh] = sink_weight * inverse
        put_heads(0, kh, mm(weights.astype(BF), values, 1, 0))

    def share(group):
        return Gather(lambda r, i: gc.at[group, i, r], 4, right, left)

    shares = {0: share(0)}
    d_gather.wait_near()
    for ry in (1, 3):
        project_grad(ry)
        for h in range(2):
            dc[ry, h, 0] = dg[ry, h, x]
    d_gather.wait_far()
    project_grad(2)
    for h in range(2):
        dc[2, h, 0] = dg[2, h, x]
    grads[...] = dacc[...].astype(BF)

    shares[0].forward()
    lane = lax.broadcasted_iota(jnp.int32, (8, 128), 1)
    sink_tile = jnp.zeros((8, 128), F32)
    for kh in range(2):
        keys = band[:, kh * HEAD : (kh + 1) * HEAD]
        values = band[:, KC + kh * HEAD : KC + (kh + 1) * HEAD]
        query = heads(queries, kh)
        grad = heads(grads, kh)
        attended = jnp.concatenate([gc[0, 2 * kh, 0], gc[0, 2 * kh + 1, 0]], axis=0)
        row_dots = jnp.sum(grad.astype(F32) * attended.astype(F32), axis=1, keepdims=True)
        weights = soft[kh]
        prob_grads = mm(grad, values, 1, 1)
        score_grads = (weights * (prob_grads - row_dots)).astype(BF)
        put_heads(1, kh, mm(score_grads, keys, 1, 0) * SCALING)
        kvg[:, kh * HEAD : (kh + 1) * HEAD] = mm(score_grads, query, 0, 0) * SCALING
        kvg[:, KC + kh * HEAD : KC + (kh + 1) * HEAD] = mm(weights.astype(BF), grad, 0, 0)
        sink_rows = psink[kh] * row_dots
        for g in range(2):
            total = -jnp.sum(sink_rows[g * TOK : (g + 1) * TOK], axis=0, keepdims=True)
            sink_tile = jnp.where(lane == 2 * kh + g, total, sink_tile)
    hs[0] = kvg[0:WINDOW, :].astype(BF)
    hs[1] = kvg[WINDOW + TOK : BAND, :].astype(BF)
    back = send(hs.at[0], hr.at[0], before)
    forth = send(hs.at[1], hr.at[1], after)
    skx[x] = sink_tile

    def owner(step):
        return pl.ds(pl.multiple_of(lax.rem(y + step, NY) * 1024, 1024), 1024)

    def own_grads(group):
        return jnp.concatenate([gc[group, k, 0] for k in range(4)], axis=1)

    def input_share(step):
        own = own_grads(2)
        return (
            dxo[step]
            + mm(own[:, :KC], wk[owner(step), :], 1, 1)
            + mm(own[:, KC:], wv[owner(step), :], 1, 1)
        )

    low, high = pl.ds(0, TOK // 2), pl.ds(TOK // 2, TOK // 2)

    def input_far():
        ys[1] = input_share(2).astype(BF)
        return [
            send(ys.at[1, low], yrelay.at[0], up),
            send(ys.at[1, high], yrelay.at[1], down),
        ]

    def input_near(step, block, rows, device):
        dxo[step] = input_share(step)
        ys[block, rows, :] = dxo[step, rows, :].astype(BF)
        return send(ys.at[block, rows], yr.at[block // 2, rows], device)

    def input_pass(copies):
        for k, step, block, rows, device in ((0, 1, 0, low, up), (1, 3, 2, high, down)):
            copies[k].wait_recv()
            ys[block, rows, :] = (dxo[step, rows, :] + yrelay[k].astype(F32)).astype(BF)
            copies.append(send(ys.at[block, rows], yr.at[block // 2, rows], device))

    shares[1] = share(1)
    sink_x = [send(skx.at[x], skx.at[x], at_x(step)) for step in (1, 3, 2)]
    dc_gather.forward()
    for copy in x_cells:
        copy.wait_recv()
    xc_gather = Gather(
        lambda ry, i: xc.at[ry, 0, pl.ds(1, 3), pl.ds(i * (TOK // 2), TOK // 2)], 2, up, down
    )
    def turn(cells, turned, blocks):
        for ry, h in blocks:
            turned[ry, h] = cells[ry, h].reshape(NX * TOK, 128).T

    for step in (2, 1, 3, 0):
        dxo[step] = mm(own_grads(1), wq[owner(step), :], 1, 1)
    turn(xc, xt, ((0, 0), (0, 1), (1, 1), (2, 1), (3, 1)))
    turn(dc, dt, ((0, 0), (0, 1), (1, 0), (3, 1)))
    shares[1].forward()
    back.wait_recv()
    forth.wait_recv()
    kvg[TOK : WINDOW + TOK, :] += hr[0].astype(F32)
    kvg[WINDOW : 2 * WINDOW, :] += hr[1].astype(F32)
    for k in range(4):
        gc[2, k, 0] = kvg[WINDOW : WINDOW + TOK, k * HEAD : (k + 1) * HEAD].astype(BF)
    shares[2] = share(2)
    dc_gather.wait_near()
    dc_gather.wait_far()
    shares[0].wait_near()
    shares[0].wait_far()

    def multiply(group, turned):
        cols = jnp.concatenate([gc[group, k].reshape(NX * TOK, 128) for k in range(4)], axis=1)

        def product(core):
            rows = pl.ds(pl.multiple_of(core * 64, 64), 64)
            left = jnp.concatenate(
                [turned[ry, h, rows, :] for ry in range(NY) for h in range(2)], axis=0
            )
            return mm(left, cols, 1, 0).reshape(NY, 2, 64, QC)

        pb[group] = product(1 - c).astype(BF)
        copy = send(pb.at[group], sr.at[group], sister)
        pf[group] = product(c)
        return copy

    class Ring:
        def __init__(self, group, from_sister, parts):
            self.group = group
            from_sister.wait_recv()
            width = QC // parts
            self.slices = [slice(p * width, (p + 1) * width) for p in range(parts)]
            self.copies = {}
            self.hop(0)

        def own(self, step, cols):
            to = lax.rem(z + step, NZ)
            ry = lax.rem(y + NY - to // 2, NY)
            h = lax.rem(to, 2)
            mine = pf[self.group, ry, h, :, cols]
            return mine + sr[self.group, ry, h, :, cols].astype(F32)

        def hop(self, k):
            for p, cols in enumerate(self.slices):
                for way, step in ((0, 4 - k), (1, 5 + k)):
                    if way == 1 and k == 3:
                        continue
                    toward = 1 if way == 0 else 7
                    if p % 2 == 1:
                        step, toward = NZ - step, NZ - toward
                    total = self.own(step, cols)
                    if k > 0:
                        self.copies[way, k - 1, p].wait_recv()
                        total = total + zr[self.group, way, k - 1, :, cols].astype(F32)
                    zs[self.group, way, k, :, cols] = total.astype(BF)
                    span = pl.ds(cols.start, cols.stop - cols.start)
                    self.copies[way, k, p] = send(
                        zs.at[self.group, way, k, :, span],
                        zr.at[self.group, way, k, :, span],
                        at_z(toward),
                    )

        def finish(self, p):
            cols = self.slices[p]
            total = self.own(0, cols)
            for way, k in ((1, 2), (0, 3)):
                self.copies[way, k, p].wait_recv()
                total = total + zr[self.group, way, k, :, cols].astype(F32)
            return total

    xc_gather.forward()
    turn(dc, dt, ((1, 1), (3, 0), (2, 0), (2, 1)))
    s0 = multiply(0, dt)
    for copy in sink_x:
        copy.wait_recv()
    skc[c] = (skx[0] + skx[1]) + (skx[2] + skx[3])
    sink_c = send(skc.at[c], skc.at[c], sister)
    ring0 = Ring(0, s0, 2)
    xc_gather.wait_near()
    xc_gather.wait_far()
    turn(xc, xt, ((1, 0), (2, 0), (3, 0)))
    shares[1].wait_near()
    shares[1].wait_far()
    shares[2].forward()
    s1 = multiply(1, xt)
    ring0.hop(1)
    ring1 = Ring(1, s1, 2)
    y_copies = input_far()
    y_copies.append(input_near(1, 0, high, up))
    shares[2].wait_near()
    shares[2].wait_far()
    s2 = multiply(2, xt)
    sink_c.wait_recv()
    skz[z] = skc[0] + skc[1]
    sink_z = []

    def sink_hop(k):
        for way, sign in ((0, -1), (1, 1)):
            if way == 1 and k == 3:
                continue
            if k > 0:
                sink_z[2 * (k - 1) + way].wait_recv()
            tile = skz.at[lax.rem(z + NZ + sign * k, NZ)]
            sink_z.append(send(tile, tile, at_z(1 if way == 0 else 7)))

    sink_hop(0)
    ring0.hop(2)
    ring2 = Ring(2, s2, 4)
    ring1.hop(1)
    y_copies.append(input_near(3, 2, low, down))
    sink_hop(1)
    ring0.hop(3)
    ring2.hop(1)
    ring1.hop(2)
    input_pass(y_copies)
    dxo[0] = input_share(0)
    sink_hop(2)
    ring2.hop(2)
    ring1.hop(3)
    sink_hop(3)
    for p, cols in enumerate(ring0.slices):
        wo_out[:, cols] = ring0.finish(p)
    ring2.hop(3)
    for copy in y_copies[2:]:
        copy.wait_recv()
    total = dxo[0]
    for k in range(2):
        total = total + yr[k].astype(F32)
    dx_out[...] = total.astype(BF)
    for p, cols in enumerate(ring1.slices):
        wq_out[:, cols] = ring1.finish(p)
    for copy in sink_z[5:]:
        copy.wait_recv()
    total = skz[0]
    for k in range(1, NZ):
        total = total + skz[k]
    sink_out[...] = total
    for p in range(2):
        wk_out[:, ring2.slices[p]] = ring2.finish(p)
        wv_out[:, ring2.slices[p]] = ring2.finish(p + 2)
    for copy in started:
        copy.wait_send()


def finish(*refs):
    for source, target in zip(refs[:5], refs[6:11]):
        target[...] = source[...]
    refs[11][...] = refs[5][0:1, 0:4]


def per_device(
    layer_input, output_grad, query_weight, key_weight, value_weight, out_weight, sink_logit
):
    vmem = pltpu.VMEM
    outside = pl.BlockSpec(memory_space=pltpu.HBM)
    inside = pl.BlockSpec(memory_space=pltpu.VMEM)
    results = (
        jax.ShapeDtypeStruct((TOK, 1024), BF),
        jax.ShapeDtypeStruct((64, QC), F32),
        jax.ShapeDtypeStruct((64, KC), F32),
        jax.ShapeDtypeStruct((64, KC), F32),
        jax.ShapeDtypeStruct((64, QC), F32),
    )
    outs = pl.pallas_call(
        kernel,
        name="attention_backward",
        out_shape=results + (jax.ShapeDtypeStruct((8, 128), F32),),
        in_specs=[outside] * 6 + [pl.BlockSpec(memory_space=pltpu.SMEM)],
        out_specs=[inside] * 6,
        scratch_shapes=[
            vmem((NY, 2, 4, TOK, 128), BF),
            vmem((NY, 2, 4, TOK, 128), BF),
            vmem((NY, 2, NX, TOK, 128), BF),
            vmem((NY, 2, NX, TOK, 128), BF),
        vmem((NY, 2, 128, NX * TOK), BF),
        vmem((NY, 2, 128, NX * TOK), BF),
            vmem((4096, QC), BF),
            vmem((4096, KC), BF),
            vmem((4096, KC), BF),
            vmem((QC, 4096), BF),
            vmem((TOK, QC + 2 * KC), F32),
            vmem((TOK, QC), F32),
            vmem((BAND, 2 * KC), BF),
            vmem((TOK, QC), BF),
            vmem((TOK, QC), BF),
            vmem((2, 2 * TOK, BAND), F32),
            vmem((2, 2 * TOK, 1), F32),
            vmem((3, 4, NX, TOK, 128), BF),
            vmem((BAND, 2 * KC), F32),
            vmem((2, WINDOW, 2 * KC), BF),
            vmem((2, WINDOW, 2 * KC), BF),
            vmem((3, NY, 2, 64, QC), F32),
            vmem((3, NY, 2, 64, QC), BF),
            vmem((3, NY, 2, 64, QC), BF),
            vmem((3, 2, 4, 64, QC), BF),
            vmem((3, 2, 4, 64, QC), BF),
            vmem((3, TOK, 1024), BF),
            vmem((2, TOK, 1024), BF),
        vmem((2, TOK // 2, 1024), BF),
            vmem((NY, TOK, 1024), F32),
            vmem((NX, 8, 128), F32),
            vmem((NC, 8, 128), F32),
            vmem((NZ, 8, 128), F32),
            pltpu.SemaphoreType.DMA((20,)),
            pltpu.SemaphoreType.DMA((COPIES,)),
            pltpu.SemaphoreType.DMA((COPIES,)),
        ],
        compiler_params=pltpu.CompilerParams(
            collective_id=0, has_side_effects=True, vmem_limit_bytes=53 * 1024 * 1024
        ),
    )(layer_input, output_grad, query_weight, key_weight, value_weight, out_weight, sink_logit)
    outs = pl.pallas_call(
        finish,
        name="finish",
        out_shape=results + (jax.ShapeDtypeStruct((1, 4), F32),),
        in_specs=[inside] * 6,
        out_specs=[inside] * 6,
        compiler_params=pltpu.CompilerParams(vmem_limit_bytes=8 * 1024 * 1024),
    )(*outs)
    return outs[:4] + (outs[4].T, outs[5].reshape(4))


def solution(mesh):
    placed = (
        P("sp", "tp"),
        P("sp", "tp"),
        P(None, "tp"),
        P(None, "tp"),
        P(None, "tp"),
        P("tp", None),
        P("tp"),
    )
    return jax.shard_map(
        per_device,
        mesh=mesh,
        in_specs=placed,
        out_specs=(
            P("sp", "tp"),
            P("sp", "tp"),
            P("sp", "tp"),
            P("sp", "tp"),
            P("tp", "sp"),
            P("tp"),
        ),
        check_vma=False,
    )
```

```python
import jax
import jax.numpy as jnp
from jax import lax
from jax.experimental import pallas as pl
from jax.experimental.pallas import tpu as pltpu
from jax.sharding import PartitionSpec as P

HEAD = 128
WINDOW = 128
NZ, NX, NC, NY = 8, 4, 2, 4
TOK = 160
SEQ = TOK * NZ * NX * NC
BAND = TOK + 2 * WINDOW
QC = 512
KC = 256
SCALING = HEAD ** (-0.5)
MASKED = -1e30
BF = jnp.bfloat16
F32 = jnp.float32
COPIES = 176


def mm(left, right, left_dim, right_dim):
    return lax.dot_general(
        left, right, (((left_dim,), (right_dim,)), ((), ())), preferred_element_type=F32
    )


def kernel(
    x_hbm, g_hbm, wq_hbm, wk_hbm, wv_hbm, wo_hbm, sink_ref,
    dx_out, wq_out, wk_out, wv_out, wo_out, sink_out,
    xg, dg, xc, dc, xt, dt, wq, wk, wv, wo, acc, dacc, band, queries, grads,
    soft, psink, gc, kvg, hs, hr, pf, pb, sr, zs, zr, ys, yr, yrelay, dxo, skx, skc, skz,
    local_sem, send_sem, recv_sem,
):
    sp = lax.axis_index("sp")
    y = lax.axis_index("tp")
    z = sp // (NX * NC)
    x = lax.rem(sp // NC, NX)
    c = lax.rem(sp, NC)

    def at_y(step):
        return (sp, lax.rem(y + step, NY))

    def at_x(step):
        return ((z * NX + lax.rem(x + step, NX)) * NC + c, y)

    def at_z(step):
        return ((lax.rem(z + step, NZ) * NX + x) * NC + c, y)

    sister = (sp + 1 - 2 * c, y)
    after = (lax.rem(sp + 1, NZ * NX * NC), y)
    before = (lax.rem(sp + NZ * NX * NC - 1, NZ * NX * NC), y)
    up, down = at_y(1), at_y(3)
    right, left = at_x(1), at_x(3)

    started = []
    local_count = [0]

    def send(src, dst, device):
        k = len(started)
        copy = pltpu.make_async_remote_copy(
            src_ref=src,
            dst_ref=dst,
            send_sem=send_sem.at[k],
            recv_sem=recv_sem.at[k],
            device_id=device,
            device_id_type=pl.DeviceIdType.MESH,
        )
        copy.start()
        started.append(copy)
        return copy

    def load(src, dst):
        k = local_count[0]
        local_count[0] += 1
        copy = pltpu.make_async_copy(src, dst, local_sem.at[k])
        copy.start()
        return copy

    def loads(hbm, blocks):
        return [
            load(hbm.at[:, pl.ds(k * 128, 128)], blocks.at[0, k // 4, k % 4]) for k in range(8)
        ]

    x_loads = loads(x_hbm, xg)
    d_loads = loads(g_hbm, dg)
    weight_loads = [load(wq_hbm, wq), load(wk_hbm, wk), load(wv_hbm, wv)]
    out_load = load(wo_hbm, wo)

    barrier = pltpu.get_barrier_semaphore()
    peers = [up, down, right, left, at_x(2), sister, after, before, at_z(1), at_z(7)]
    for peer in peers:
        pl.semaphore_signal(
            barrier, inc=1, device_id=peer, device_id_type=pl.DeviceIdType.MESH
        )
    pl.semaphore_wait(barrier, len(peers))

    class Gather:
        def __init__(self, piece, count, plus, minus):
            self.piece, self.count, self.plus, self.minus = piece, count, plus, minus
            self.ahead, self.behind, self.far = {}, {}, []
            for i in range(count):
                k = count - 1 - i
                self.ahead[i] = send(piece(0, i), piece(1, i), plus)
                self.behind[k] = send(piece(0, k), piece(3, k), minus)

        def forward(self):
            for i in range(self.count // 2):
                k = self.count - 1 - i
                self.ahead[i].wait_recv()
                self.far.append(send(self.piece(1, i), self.piece(2, i), self.plus))
                self.behind[k].wait_recv()
                self.far.append(send(self.piece(3, k), self.piece(2, k), self.minus))

        def wait_near(self):
            for i in range(self.count // 2, self.count):
                self.ahead[i].wait_recv()
                self.behind[self.count - 1 - i].wait_recv()

        def wait_far(self):
            for copy in self.far:
                copy.wait_recv()

    def quarters(blocks):
        return lambda ry, i: blocks.at[ry, i // 2, pl.ds(2 * (i % 2), 2)]

    def exchange(blocks, cells, ry):
        copies = [
            send(blocks.at[ry, :, lax.rem(x + step, NX)], cells.at[ry, :, step], at_x(step))
            for step in ((2, 1, 3) if ry == 0 else (1, 3))
        ]
        for h in range(2):
            cells[ry, h, 0] = blocks[ry, h, x]
        return copies

    def wide(blocks, ry):
        return jnp.concatenate([blocks[ry, h, k] for h in range(2) for k in range(4)], axis=1)

    def features(ry):
        return pl.multiple_of(lax.rem(y + NY - ry, NY) * 1024, 1024)

    def project(ry):
        rows = pl.ds(features(ry), 1024)
        block = wide(xg, ry)
        for cols, weight in (
            (slice(0, QC), wq),
            (slice(QC, QC + KC), wk),
            (slice(QC + KC, QC + 2 * KC), wv),
        ):
            term = mm(block, weight[rows, :], 1, 0)
            acc[:, cols] = term if ry == 0 else acc[:, cols] + term

    def project_grad(ry):
        cols = pl.ds(features(ry), 1024)
        term = mm(wide(dg, ry), wo[:, cols], 1, 1)
        dacc[...] = term if ry == 0 else dacc[...] + term

    for copy in x_loads:
        copy.wait()
    x_gather = Gather(quarters(xg), 4, up, down)
    x_cells = exchange(xg, xc, 0)
    for copy in d_loads:
        copy.wait()
    d_cells = exchange(dg, dc, 0)
    for copy in weight_loads:
        copy.wait()
    project(0)
    x_gather.forward()
    d_gather = Gather(quarters(dg), 4, up, down)
    x_gather.wait_near()
    x_cells += exchange(xg, xc, 1)
    x_cells += exchange(xg, xc, 3)
    project(1)
    project(3)
    x_gather.wait_far()
    project(2)

    band[WINDOW : WINDOW + TOK, :] = acc[:, QC : QC + 2 * KC].astype(BF)
    queries[...] = acc[:, :QC].astype(BF)
    halo_after = send(band.at[pl.ds(TOK, WINDOW)], band.at[pl.ds(0, WINDOW)], after)
    halo_before = send(
        band.at[pl.ds(WINDOW, WINDOW)], band.at[pl.ds(WINDOW + TOK, WINDOW)], before
    )
    x_cells += exchange(xg, xc, 2)
    d_gather.forward()
    for copy in d_cells:
        copy.wait_recv()
    dc_gather = Gather(lambda ry, h: dc.at[ry, h, pl.ds(1, 3)], 2, up, down)
    out_load.wait()
    project_grad(0)
    halo_after.wait_recv()
    halo_before.wait_recv()

    row = lax.broadcasted_iota(jnp.int32, (2 * TOK, BAND), 0)
    row = jnp.where(row >= TOK, row - TOK, row)
    col = lax.broadcasted_iota(jnp.int32, (2 * TOK, BAND), 1) - WINDOW
    key_pos = sp * TOK + col
    in_window = (jnp.abs(row - col) <= WINDOW) & (key_pos >= 0) & (key_pos < SEQ)
    second_head = lax.broadcasted_iota(jnp.int32, (2 * TOK, 1), 0) >= TOK

    def heads(ref, kh):
        cols = kh * 2 * HEAD
        return jnp.concatenate(
            [ref[:, cols : cols + HEAD], ref[:, cols + HEAD : cols + 2 * HEAD]], axis=0
        )

    def put_heads(group, kh, value):
        gc[group, 2 * kh, 0] = value[:TOK].astype(BF)
        gc[group, 2 * kh + 1, 0] = value[TOK:].astype(BF)

    for kh in range(2):
        keys = band[:, kh * HEAD : (kh + 1) * HEAD]
        values = band[:, KC + kh * HEAD : KC + (kh + 1) * HEAD]
        scores = mm(heads(queries, kh), keys, 1, 1) * SCALING
        scores = jnp.where(in_window, scores, MASKED)
        sink = jnp.where(second_head, sink_ref[2 * kh + 1], sink_ref[2 * kh])
        row_max = jnp.maximum(jnp.max(scores, axis=1, keepdims=True), sink)
        weights = jnp.exp(scores - row_max)
        sink_weight = jnp.exp(sink - row_max)
        inverse = 1.0 / (jnp.sum(weights, axis=1, keepdims=True) + sink_weight)
        weights = weights * inverse
        soft[kh] = weights
        psink[kh] = sink_weight * inverse
        put_heads(0, kh, mm(weights.astype(BF), values, 1, 0))

    def share(group):
        return Gather(lambda r, i: gc.at[group, i, r], 4, right, left)

    shares = {0: share(0)}
    d_gather.wait_near()
    for ry in (1, 3):
        project_grad(ry)
        for h in range(2):
            dc[ry, h, 0] = dg[ry, h, x]
    d_gather.wait_far()
    project_grad(2)
    for h in range(2):
        dc[2, h, 0] = dg[2, h, x]
    grads[...] = dacc[...].astype(BF)

    shares[0].forward()
    lane = lax.broadcasted_iota(jnp.int32, (8, 128), 1)
    sink_tile = jnp.zeros((8, 128), F32)
    for kh in range(2):
        keys = band[:, kh * HEAD : (kh + 1) * HEAD]
        values = band[:, KC + kh * HEAD : KC + (kh + 1) * HEAD]
        query = heads(queries, kh)
        grad = heads(grads, kh)
        attended = jnp.concatenate([gc[0, 2 * kh, 0], gc[0, 2 * kh + 1, 0]], axis=0)
        row_dots = jnp.sum(grad.astype(F32) * attended.astype(F32), axis=1, keepdims=True)
        weights = soft[kh]
        prob_grads = mm(grad, values, 1, 1)
        score_grads = (weights * (prob_grads - row_dots)).astype(BF)
        put_heads(1, kh, mm(score_grads, keys, 1, 0) * SCALING)
        kvg[:, kh * HEAD : (kh + 1) * HEAD] = mm(score_grads, query, 0, 0) * SCALING
        kvg[:, KC + kh * HEAD : KC + (kh + 1) * HEAD] = mm(weights.astype(BF), grad, 0, 0)
        sink_rows = psink[kh] * row_dots
        for g in range(2):
            total = -jnp.sum(sink_rows[g * TOK : (g + 1) * TOK], axis=0, keepdims=True)
            sink_tile = jnp.where(lane == 2 * kh + g, total, sink_tile)
    hs[0] = kvg[0:WINDOW, :].astype(BF)
    hs[1] = kvg[WINDOW + TOK : BAND, :].astype(BF)
    back = send(hs.at[0], hr.at[0], before)
    forth = send(hs.at[1], hr.at[1], after)
    skx[x] = sink_tile

    def owner(step):
        return pl.ds(pl.multiple_of(lax.rem(y + step, NY) * 1024, 1024), 1024)

    def own_grads(group):
        return jnp.concatenate([gc[group, k, 0] for k in range(4)], axis=1)

    def input_share(step):
        own = own_grads(2)
        return (
            dxo[step]
            + mm(own[:, :KC], wk[owner(step), :], 1, 1)
            + mm(own[:, KC:], wv[owner(step), :], 1, 1)
        )

    low, high = pl.ds(0, TOK // 2), pl.ds(TOK // 2, TOK // 2)

    def input_far():
        ys[1] = input_share(2).astype(BF)
        return [
            send(ys.at[1, low], yrelay.at[0], up),
            send(ys.at[1, high], yrelay.at[1], down),
        ]

    def input_near(step, block, rows, device):
        dxo[step] = input_share(step)
        ys[block, rows, :] = dxo[step, rows, :].astype(BF)
        return send(ys.at[block, rows], yr.at[block // 2, rows], device)

    def input_pass(copies):
        for k, step, block, rows, device in ((0, 1, 0, low, up), (1, 3, 2, high, down)):
            copies[k].wait_recv()
            ys[block, rows, :] = (dxo[step, rows, :] + yrelay[k].astype(F32)).astype(BF)
            copies.append(send(ys.at[block, rows], yr.at[block // 2, rows], device))

    shares[1] = share(1)
    sink_x = [send(skx.at[x], skx.at[x], at_x(step)) for step in (1, 3, 2)]
    dc_gather.forward()
    for copy in x_cells:
        copy.wait_recv()
    xc_gather = Gather(lambda ry, h: xc.at[ry, h, 2], 2, up, down)
    def turn(cells, turned, blocks):
        for ry, h in blocks:
            turned[ry, h] = cells[ry, h].reshape(NX * TOK, 128).T

    for step in (2, 1, 3, 0):
        dxo[step] = mm(own_grads(1), wq[owner(step), :], 1, 1)
    turn(xc, xt, ((0, 0), (0, 1)))
    turn(dc, dt, ((0, 0), (0, 1), (1, 0), (3, 1)))
    shares[1].forward()
    back.wait_recv()
    forth.wait_recv()
    kvg[TOK : WINDOW + TOK, :] += hr[0].astype(F32)
    kvg[WINDOW : 2 * WINDOW, :] += hr[1].astype(F32)
    for k in range(4):
        gc[2, k, 0] = kvg[WINDOW : WINDOW + TOK, k * HEAD : (k + 1) * HEAD].astype(BF)
    shares[2] = share(2)
    dc_gather.wait_near()
    dc_gather.wait_far()
    shares[0].wait_near()
    shares[0].wait_far()

    def multiply(group, turned):
        cols = jnp.concatenate([gc[group, k].reshape(NX * TOK, 128) for k in range(4)], axis=1)

        def product(core):
            rows = pl.ds(pl.multiple_of(core * 64, 64), 64)
            left = jnp.concatenate(
                [turned[ry, h, rows, :] for ry in range(NY) for h in range(2)], axis=0
            )
            return mm(left, cols, 1, 0).reshape(NY, 2, 64, QC)

        pb[group] = product(1 - c).astype(BF)
        copy = send(pb.at[group], sr.at[group], sister)
        pf[group] = product(c)
        return copy

    class Ring:
        def __init__(self, group, from_sister, parts):
            self.group = group
            from_sister.wait_recv()
            width = QC // parts
            self.slices = [slice(p * width, (p + 1) * width) for p in range(parts)]
            self.copies = {}
            self.hop(0)

        def own(self, step, cols):
            to = lax.rem(z + step, NZ)
            ry = lax.rem(y + NY - to // 2, NY)
            h = lax.rem(to, 2)
            mine = pf[self.group, ry, h, :, cols]
            return mine + sr[self.group, ry, h, :, cols].astype(F32)

        def hop(self, k):
            for p, cols in enumerate(self.slices):
                for way, step in ((0, 4 - k), (1, 5 + k)):
                    if way == 1 and k == 3:
                        continue
                    toward = 1 if way == 0 else 7
                    if p % 2 == 1:
                        step, toward = NZ - step, NZ - toward
                    total = self.own(step, cols)
                    if k > 0:
                        self.copies[way, k - 1, p].wait_recv()
                        total = total + zr[self.group, way, k - 1, :, cols].astype(F32)
                    zs[self.group, way, k, :, cols] = total.astype(BF)
                    span = pl.ds(cols.start, cols.stop - cols.start)
                    self.copies[way, k, p] = send(
                        zs.at[self.group, way, k, :, span],
                        zr.at[self.group, way, k, :, span],
                        at_z(toward),
                    )

        def finish(self, p):
            cols = self.slices[p]
            total = self.own(0, cols)
            for way, k in ((1, 2), (0, 3)):
                self.copies[way, k, p].wait_recv()
                total = total + zr[self.group, way, k, :, cols].astype(F32)
            return total

    xc_gather.forward()
    turn(dc, dt, ((1, 1), (3, 0), (2, 0), (2, 1)))
    s0 = multiply(0, dt)
    for copy in sink_x:
        copy.wait_recv()
    skc[c] = (skx[0] + skx[1]) + (skx[2] + skx[3])
    sink_c = send(skc.at[c], skc.at[c], sister)
    ring0 = Ring(0, s0, 2)
    xc_gather.wait_near()
    xc_gather.wait_far()
    turn(xc, xt, [(ry, h) for ry in (1, 2, 3) for h in range(2)])
    shares[1].wait_near()
    shares[1].wait_far()
    shares[2].forward()
    s1 = multiply(1, xt)
    ring0.hop(1)
    ring1 = Ring(1, s1, 2)
    y_copies = input_far()
    y_copies.append(input_near(1, 0, high, up))
    shares[2].wait_near()
    shares[2].wait_far()
    s2 = multiply(2, xt)
    sink_c.wait_recv()
    skz[z] = skc[0] + skc[1]
    sink_z = []

    def sink_hop(k):
        for way, sign in ((0, -1), (1, 1)):
            if way == 1 and k == 3:
                continue
            if k > 0:
                sink_z[2 * (k - 1) + way].wait_recv()
            tile = skz.at[lax.rem(z + NZ + sign * k, NZ)]
            sink_z.append(send(tile, tile, at_z(1 if way == 0 else 7)))

    sink_hop(0)
    ring0.hop(2)
    ring2 = Ring(2, s2, 4)
    ring1.hop(1)
    y_copies.append(input_near(3, 2, low, down))
    sink_hop(1)
    ring0.hop(3)
    ring2.hop(1)
    ring1.hop(2)
    input_pass(y_copies)
    dxo[0] = input_share(0)
    sink_hop(2)
    ring2.hop(2)
    ring1.hop(3)
    sink_hop(3)
    for p, cols in enumerate(ring0.slices):
        wo_out[:, cols] = ring0.finish(p)
    ring2.hop(3)
    for copy in y_copies[2:]:
        copy.wait_recv()
    total = dxo[0]
    for k in range(2):
        total = total + yr[k].astype(F32)
    dx_out[...] = total.astype(BF)
    for p, cols in enumerate(ring1.slices):
        wq_out[:, cols] = ring1.finish(p)
    for copy in sink_z[5:]:
        copy.wait_recv()
    total = skz[0]
    for k in range(1, NZ):
        total = total + skz[k]
    sink_out[...] = total
    for p in range(2):
        wk_out[:, ring2.slices[p]] = ring2.finish(p)
        wv_out[:, ring2.slices[p]] = ring2.finish(p + 2)
    for copy in started:
        copy.wait_send()


def finish(*refs):
    for source, target in zip(refs[:5], refs[6:11]):
        target[...] = source[...]
    refs[11][...] = refs[5][0:1, 0:4]


def per_device(
    layer_input, output_grad, query_weight, key_weight, value_weight, out_weight, sink_logit
):
    vmem = pltpu.VMEM
    outside = pl.BlockSpec(memory_space=pltpu.HBM)
    inside = pl.BlockSpec(memory_space=pltpu.VMEM)
    results = (
        jax.ShapeDtypeStruct((TOK, 1024), BF),
        jax.ShapeDtypeStruct((64, QC), F32),
        jax.ShapeDtypeStruct((64, KC), F32),
        jax.ShapeDtypeStruct((64, KC), F32),
        jax.ShapeDtypeStruct((64, QC), F32),
    )
    outs = pl.pallas_call(
        kernel,
        name="attention_backward",
        out_shape=results + (jax.ShapeDtypeStruct((8, 128), F32),),
        in_specs=[outside] * 6 + [pl.BlockSpec(memory_space=pltpu.SMEM)],
        out_specs=[inside] * 6,
        scratch_shapes=[
            vmem((NY, 2, 4, TOK, 128), BF),
            vmem((NY, 2, 4, TOK, 128), BF),
            vmem((NY, 2, NX, TOK, 128), BF),
            vmem((NY, 2, NX, TOK, 128), BF),
        vmem((NY, 2, 128, NX * TOK), BF),
        vmem((NY, 2, 128, NX * TOK), BF),
            vmem((4096, QC), BF),
            vmem((4096, KC), BF),
            vmem((4096, KC), BF),
            vmem((QC, 4096), BF),
            vmem((TOK, QC + 2 * KC), F32),
            vmem((TOK, QC), F32),
            vmem((BAND, 2 * KC), BF),
            vmem((TOK, QC), BF),
            vmem((TOK, QC), BF),
            vmem((2, 2 * TOK, BAND), F32),
            vmem((2, 2 * TOK, 1), F32),
            vmem((3, 4, NX, TOK, 128), BF),
            vmem((BAND, 2 * KC), F32),
            vmem((2, WINDOW, 2 * KC), BF),
            vmem((2, WINDOW, 2 * KC), BF),
            vmem((3, NY, 2, 64, QC), F32),
            vmem((3, NY, 2, 64, QC), BF),
            vmem((3, NY, 2, 64, QC), BF),
            vmem((3, 2, 4, 64, QC), BF),
            vmem((3, 2, 4, 64, QC), BF),
            vmem((3, TOK, 1024), BF),
            vmem((2, TOK, 1024), BF),
        vmem((2, TOK // 2, 1024), BF),
            vmem((NY, TOK, 1024), F32),
            vmem((NX, 8, 128), F32),
            vmem((NC, 8, 128), F32),
            vmem((NZ, 8, 128), F32),
            pltpu.SemaphoreType.DMA((20,)),
            pltpu.SemaphoreType.DMA((COPIES,)),
            pltpu.SemaphoreType.DMA((COPIES,)),
        ],
        compiler_params=pltpu.CompilerParams(
            collective_id=0, has_side_effects=True, vmem_limit_bytes=53 * 1024 * 1024
        ),
    )(layer_input, output_grad, query_weight, key_weight, value_weight, out_weight, sink_logit)
    outs = pl.pallas_call(
        finish,
        name="finish",
        out_shape=results + (jax.ShapeDtypeStruct((1, 4), F32),),
        in_specs=[inside] * 6,
        out_specs=[inside] * 6,
        compiler_params=pltpu.CompilerParams(vmem_limit_bytes=8 * 1024 * 1024),
    )(*outs)
    return outs[:4] + (outs[4].T, outs[5].reshape(4))


def solution(mesh):
    placed = (
        P("sp", "tp"),
        P("sp", "tp"),
        P(None, "tp"),
        P(None, "tp"),
        P(None, "tp"),
        P("tp", None),
        P("tp"),
    )
    return jax.shard_map(
        per_device,
        mesh=mesh,
        in_specs=placed,
        out_specs=(
            P("sp", "tp"),
            P("sp", "tp"),
            P("sp", "tp"),
            P("sp", "tp"),
            P("tp", "sp"),
            P("tp"),
        ),
        check_vma=False,
    )
```

```python
import jax
import jax.numpy as jnp
from jax import lax
from jax.experimental import pallas as pl
from jax.experimental.pallas import tpu as pltpu
from jax.sharding import PartitionSpec as P

HEAD = 128
WINDOW = 128
NZ, NX, NC, NY = 8, 4, 2, 4
TOK = 160
SEQ = TOK * NZ * NX * NC
BAND = TOK + 2 * WINDOW
QC = 512
KC = 256
SCALING = HEAD ** (-0.5)
MASKED = -1e30
BF = jnp.bfloat16
F32 = jnp.float32
COPIES = 176


def mm(left, right, left_dim, right_dim):
    return lax.dot_general(
        left, right, (((left_dim,), (right_dim,)), ((), ())), preferred_element_type=F32
    )


def kernel(
    x_hbm, g_hbm, wq_hbm, wk_hbm, wv_hbm, wo_hbm, sink_ref,
    dx_out, wq_out, wk_out, wv_out, wo_out, sink_out,
    xg, dg, xc, dc, xt, dt, wq, wk, wv, wo, acc, dacc, band, queries, grads,
    soft, psink, bias, gc, kvg, hs, hr, pf, pb, sr, zs, zr, ys, yr, yrelay, dxo, skx, skc, skz,
    local_sem, send_sem, recv_sem,
):
    sp = lax.axis_index("sp")
    y = lax.axis_index("tp")
    z = sp // (NX * NC)
    x = lax.rem(sp // NC, NX)
    c = lax.rem(sp, NC)

    def at_y(step):
        return (sp, lax.rem(y + step, NY))

    def at_x(step):
        return ((z * NX + lax.rem(x + step, NX)) * NC + c, y)

    def at_z(step):
        return ((lax.rem(z + step, NZ) * NX + x) * NC + c, y)

    sister = (sp + 1 - 2 * c, y)
    after = (lax.rem(sp + 1, NZ * NX * NC), y)
    before = (lax.rem(sp + NZ * NX * NC - 1, NZ * NX * NC), y)
    up, down = at_y(1), at_y(3)
    right, left = at_x(1), at_x(3)

    started = []
    local_count = [0]

    def send(src, dst, device):
        k = len(started)
        copy = pltpu.make_async_remote_copy(
            src_ref=src,
            dst_ref=dst,
            send_sem=send_sem.at[k],
            recv_sem=recv_sem.at[k],
            device_id=device,
            device_id_type=pl.DeviceIdType.MESH,
        )
        copy.start()
        started.append(copy)
        return copy

    def load(src, dst):
        k = local_count[0]
        local_count[0] += 1
        copy = pltpu.make_async_copy(src, dst, local_sem.at[k])
        copy.start()
        return copy

    def loads(hbm, blocks):
        return [
            load(hbm.at[:, pl.ds(k * 128, 128)], blocks.at[0, k // 4, k % 4]) for k in range(8)
        ]

    x_loads = loads(x_hbm, xg)
    d_loads = loads(g_hbm, dg)
    weight_loads = [load(wq_hbm, wq), load(wk_hbm, wk), load(wv_hbm, wv)]
    out_load = load(wo_hbm, wo)

    barrier = pltpu.get_barrier_semaphore()
    peers = [up, down, right, left, at_x(2), sister, after, before, at_z(1), at_z(7)]
    for peer in peers:
        pl.semaphore_signal(
            barrier, inc=1, device_id=peer, device_id_type=pl.DeviceIdType.MESH
        )
    pl.semaphore_wait(barrier, len(peers))

    class Gather:
        def __init__(self, piece, count, plus, minus):
            self.piece, self.count, self.plus, self.minus = piece, count, plus, minus
            self.ahead, self.behind, self.far = {}, {}, []
            for i in range(count):
                k = count - 1 - i
                self.ahead[i] = send(piece(0, i), piece(1, i), plus)
                self.behind[k] = send(piece(0, k), piece(3, k), minus)

        def forward(self):
            for i in range(self.count // 2):
                k = self.count - 1 - i
                self.ahead[i].wait_recv()
                self.far.append(send(self.piece(1, i), self.piece(2, i), self.plus))
                self.behind[k].wait_recv()
                self.far.append(send(self.piece(3, k), self.piece(2, k), self.minus))

        def wait_near(self):
            for i in range(self.count // 2, self.count):
                self.ahead[i].wait_recv()
                self.behind[self.count - 1 - i].wait_recv()

        def wait_far(self):
            for copy in self.far:
                copy.wait_recv()

    def quarters(blocks):
        return lambda ry, i: blocks.at[ry, i // 2, pl.ds(2 * (i % 2), 2)]

    def exchange(blocks, cells, ry):
        copies = [
            send(blocks.at[ry, :, lax.rem(x + step, NX)], cells.at[ry, :, step], at_x(step))
            for step in ((2, 1, 3) if ry == 0 else (1, 3))
        ]
        for h in range(2):
            cells[ry, h, 0] = blocks[ry, h, x]
        return copies

    def wide(blocks, ry):
        return jnp.concatenate([blocks[ry, h, k] for h in range(2) for k in range(4)], axis=1)

    def features(ry):
        return pl.multiple_of(lax.rem(y + NY - ry, NY) * 1024, 1024)

    def project(ry):
        rows = pl.ds(features(ry), 1024)
        block = wide(xg, ry)
        for cols, weight in (
            (slice(0, QC), wq),
            (slice(QC, QC + KC), wk),
            (slice(QC + KC, QC + 2 * KC), wv),
        ):
            term = mm(block, weight[rows, :], 1, 0)
            acc[:, cols] = term if ry == 0 else acc[:, cols] + term

    def project_grad(ry):
        cols = pl.ds(features(ry), 1024)
        term = mm(wide(dg, ry), wo[:, cols], 1, 1)
        dacc[...] = term if ry == 0 else dacc[...] + term

    for copy in x_loads:
        copy.wait()
    x_gather = Gather(quarters(xg), 4, up, down)
    x_cells = exchange(xg, xc, 0)
    for copy in d_loads:
        copy.wait()
    d_cells = exchange(dg, dc, 0)
    for copy in weight_loads:
        copy.wait()
    project(0)
    x_gather.forward()
    d_gather = Gather(quarters(dg), 4, up, down)
    x_gather.wait_near()
    x_cells += exchange(xg, xc, 1)
    x_cells += exchange(xg, xc, 3)
    project(1)
    project(3)
    x_gather.wait_far()
    project(2)

    band[WINDOW : WINDOW + TOK, :] = acc[:, QC : QC + 2 * KC].astype(BF)
    queries[...] = acc[:, :QC].astype(BF)
    halo_after = send(band.at[pl.ds(TOK, WINDOW)], band.at[pl.ds(0, WINDOW)], after)
    halo_before = send(
        band.at[pl.ds(WINDOW, WINDOW)], band.at[pl.ds(WINDOW + TOK, WINDOW)], before
    )
    x_cells += exchange(xg, xc, 2)
    d_gather.forward()
    for copy in d_cells:
        copy.wait_recv()
    dc_gather = Gather(lambda ry, h: dc.at[ry, h, pl.ds(1, 3)], 2, up, down)
    out_load.wait()
    project_grad(0)
    row = lax.broadcasted_iota(jnp.int32, (2 * TOK, BAND), 0)
    row = jnp.where(row >= TOK, row - TOK, row)
    col = lax.broadcasted_iota(jnp.int32, (2 * TOK, BAND), 1) - WINDOW
    key_pos = sp * TOK + col
    in_window = (jnp.abs(row - col) <= WINDOW) & (key_pos >= 0) & (key_pos < SEQ)
    bias[...] = jnp.where(in_window, 0.0, MASKED)
    second_head = lax.broadcasted_iota(jnp.int32, (2 * TOK, 1), 0) >= TOK

    def heads(ref, kh):
        cols = kh * 2 * HEAD
        return jnp.concatenate(
            [ref[:, cols : cols + HEAD], ref[:, cols + HEAD : cols + 2 * HEAD]], axis=0
        )

    def put_heads(group, kh, value):
        gc[group, 2 * kh, 0] = value[:TOK].astype(BF)
        gc[group, 2 * kh + 1, 0] = value[TOK:].astype(BF)

    halo_after.wait_recv()
    halo_before.wait_recv()

    for kh in range(2):
        keys = band[:, kh * HEAD : (kh + 1) * HEAD]
        values = band[:, KC + kh * HEAD : KC + (kh + 1) * HEAD]
        scores = mm(heads(queries, kh), keys, 1, 1) * SCALING
        scores = jnp.where(bias[...] < 0.0, MASKED, scores)
        sink = jnp.where(second_head, sink_ref[2 * kh + 1], sink_ref[2 * kh])
        row_max = jnp.maximum(jnp.max(scores, axis=1, keepdims=True), sink)
        weights = jnp.exp(scores - row_max)
        sink_weight = jnp.exp(sink - row_max)
        inverse = 1.0 / (jnp.sum(weights, axis=1, keepdims=True) + sink_weight)
        weights = weights * inverse
        soft[kh] = weights
        psink[kh] = sink_weight * inverse
        put_heads(0, kh, mm(weights.astype(BF), values, 1, 0))

    def share(group):
        return Gather(lambda r, i: gc.at[group, i, r], 4, right, left)

    shares = {0: share(0)}
    d_gather.wait_near()
    for ry in (1, 3):
        project_grad(ry)
        for h in range(2):
            dc[ry, h, 0] = dg[ry, h, x]
    d_gather.wait_far()
    project_grad(2)
    for h in range(2):
        dc[2, h, 0] = dg[2, h, x]
    grads[...] = dacc[...].astype(BF)

    shares[0].forward()
    lane = lax.broadcasted_iota(jnp.int32, (8, 128), 1)
    sink_tile = jnp.zeros((8, 128), F32)
    for kh in range(2):
        keys = band[:, kh * HEAD : (kh + 1) * HEAD]
        values = band[:, KC + kh * HEAD : KC + (kh + 1) * HEAD]
        query = heads(queries, kh)
        grad = heads(grads, kh)
        attended = jnp.concatenate([gc[0, 2 * kh, 0], gc[0, 2 * kh + 1, 0]], axis=0)
        row_dots = jnp.sum(grad.astype(F32) * attended.astype(F32), axis=1, keepdims=True)
        weights = soft[kh]
        prob_grads = mm(grad, values, 1, 1)
        score_grads = (weights * (prob_grads - row_dots)).astype(BF)
        put_heads(1, kh, mm(score_grads, keys, 1, 0) * SCALING)
        kvg[:, kh * HEAD : (kh + 1) * HEAD] = mm(score_grads, query, 0, 0) * SCALING
        kvg[:, KC + kh * HEAD : KC + (kh + 1) * HEAD] = mm(weights.astype(BF), grad, 0, 0)
        sink_rows = psink[kh] * row_dots
        for g in range(2):
            total = -jnp.sum(sink_rows[g * TOK : (g + 1) * TOK], axis=0, keepdims=True)
            sink_tile = jnp.where(lane == 2 * kh + g, total, sink_tile)
    hs[0] = kvg[0:WINDOW, :].astype(BF)
    hs[1] = kvg[WINDOW + TOK : BAND, :].astype(BF)
    back = send(hs.at[0], hr.at[0], before)
    forth = send(hs.at[1], hr.at[1], after)
    skx[x] = sink_tile

    def owner(step):
        return pl.ds(pl.multiple_of(lax.rem(y + step, NY) * 1024, 1024), 1024)

    def own_grads(group):
        return jnp.concatenate([gc[group, k, 0] for k in range(4)], axis=1)

    def input_share(step):
        own = own_grads(2)
        return (
            dxo[step]
            + mm(own[:, :KC], wk[owner(step), :], 1, 1)
            + mm(own[:, KC:], wv[owner(step), :], 1, 1)
        )

    low, high = pl.ds(0, TOK // 2), pl.ds(TOK // 2, TOK // 2)

    def input_far():
        ys[1] = input_share(2).astype(BF)
        return [
            send(ys.at[1, low], yrelay.at[0], up),
            send(ys.at[1, high], yrelay.at[1], down),
        ]

    def input_near(step, block, rows, device):
        dxo[step] = input_share(step)
        ys[block, rows, :] = dxo[step, rows, :].astype(BF)
        return send(ys.at[block, rows], yr.at[block // 2, rows], device)

    def input_pass(copies):
        for k, step, block, rows, device in ((0, 1, 0, low, up), (1, 3, 2, high, down)):
            copies[k].wait_recv()
            ys[block, rows, :] = (dxo[step, rows, :] + yrelay[k].astype(F32)).astype(BF)
            copies.append(send(ys.at[block, rows], yr.at[block // 2, rows], device))

    shares[1] = share(1)
    sink_x = [send(skx.at[x], skx.at[x], at_x(step)) for step in (1, 3, 2)]
    dc_gather.forward()
    for copy in x_cells:
        copy.wait_recv()
    xc_gather = Gather(lambda ry, h: xc.at[ry, h, 2], 2, up, down)
    def turn(cells, turned, blocks):
        for ry, h in blocks:
            turned[ry, h] = cells[ry, h].reshape(NX * TOK, 128).T

    for step in (2, 1, 3, 0):
        dxo[step] = mm(own_grads(1), wq[owner(step), :], 1, 1)
    turn(xc, xt, ((0, 0), (0, 1)))
    turn(dc, dt, ((0, 0), (0, 1), (1, 0), (3, 1)))
    shares[1].forward()
    back.wait_recv()
    forth.wait_recv()
    kvg[TOK : WINDOW + TOK, :] += hr[0].astype(F32)
    kvg[WINDOW : 2 * WINDOW, :] += hr[1].astype(F32)
    for k in range(4):
        gc[2, k, 0] = kvg[WINDOW : WINDOW + TOK, k * HEAD : (k + 1) * HEAD].astype(BF)
    shares[2] = share(2)
    dc_gather.wait_near()
    dc_gather.wait_far()
    shares[0].wait_near()
    shares[0].wait_far()

    def multiply(group, turned, between=None):
        cols = jnp.concatenate([gc[group, k].reshape(NX * TOK, 128) for k in range(4)], axis=1)

        def product(core):
            rows = pl.ds(pl.multiple_of(core * 64, 64), 64)
            left = jnp.concatenate(
                [turned[ry, h, rows, :] for ry in range(NY) for h in range(2)], axis=0
            )
            return mm(left, cols, 1, 0).reshape(NY, 2, 64, QC)

        pb[group] = product(1 - c).astype(BF)
        copy = send(pb.at[group], sr.at[group], sister)
        if between is not None:
            between()
        pf[group] = product(c)
        return copy

    class Ring:
        def __init__(self, group, from_sister, parts):
            self.group = group
            from_sister.wait_recv()
            width = QC // parts
            self.slices = [slice(p * width, (p + 1) * width) for p in range(parts)]
            self.copies = {}
            self.hop(0)

        def own(self, step, cols):
            to = lax.rem(z + step, NZ)
            ry = lax.rem(y + NY - to // 2, NY)
            h = lax.rem(to, 2)
            mine = pf[self.group, ry, h, :, cols]
            return mine + sr[self.group, ry, h, :, cols].astype(F32)

        def hop(self, k):
            for p, cols in enumerate(self.slices):
                for way, step in ((0, 4 - k), (1, 5 + k)):
                    if way == 1 and k == 3:
                        continue
                    toward = 1 if way == 0 else 7
                    if p % 2 == 1:
                        step, toward = NZ - step, NZ - toward
                    total = self.own(step, cols)
                    if k > 0:
                        self.copies[way, k - 1, p].wait_recv()
                        total = total + zr[self.group, way, k - 1, :, cols].astype(F32)
                    zs[self.group, way, k, :, cols] = total.astype(BF)
                    span = pl.ds(cols.start, cols.stop - cols.start)
                    self.copies[way, k, p] = send(
                        zs.at[self.group, way, k, :, span],
                        zr.at[self.group, way, k, :, span],
                        at_z(toward),
                    )

        def finish(self, p):
            cols = self.slices[p]
            total = self.own(0, cols)
            for way, k in ((1, 2), (0, 3)):
                self.copies[way, k, p].wait_recv()
                total = total + zr[self.group, way, k, :, cols].astype(F32)
            return total

    turn(dc, dt, ((1, 1), (3, 0), (2, 0), (2, 1)))
    s0 = multiply(0, dt, xc_gather.forward)
    for copy in sink_x:
        copy.wait_recv()
    skc[c] = (skx[0] + skx[1]) + (skx[2] + skx[3])
    sink_c = send(skc.at[c], skc.at[c], sister)
    ring0 = Ring(0, s0, 2)
    xc_gather.wait_near()
    xc_gather.wait_far()
    turn(xc, xt, [(ry, h) for ry in (1, 2, 3) for h in range(2)])
    shares[1].wait_near()
    shares[1].wait_far()
    shares[2].forward()
    s1 = multiply(1, xt)
    ring0.hop(1)
    ring1 = Ring(1, s1, 2)
    y_copies = input_far()
    y_copies.append(input_near(1, 0, high, up))
    shares[2].wait_near()
    shares[2].wait_far()
    s2 = multiply(2, xt)
    sink_c.wait_recv()
    skz[z] = skc[0] + skc[1]
    sink_z = []

    def sink_hop(k):
        for way, sign in ((0, -1), (1, 1)):
            if way == 1 and k == 3:
                continue
            if k > 0:
                sink_z[2 * (k - 1) + way].wait_recv()
            tile = skz.at[lax.rem(z + NZ + sign * k, NZ)]
            sink_z.append(send(tile, tile, at_z(1 if way == 0 else 7)))

    sink_hop(0)
    ring0.hop(2)
    ring2 = Ring(2, s2, 4)
    ring1.hop(1)
    y_copies.append(input_near(3, 2, low, down))
    sink_hop(1)
    ring0.hop(3)
    ring2.hop(1)
    ring1.hop(2)
    input_pass(y_copies)
    dxo[0] = input_share(0)
    sink_hop(2)
    ring2.hop(2)
    ring1.hop(3)
    sink_hop(3)
    for p, cols in enumerate(ring0.slices):
        wo_out[:, cols] = ring0.finish(p)
    ring2.hop(3)
    for copy in y_copies[2:]:
        copy.wait_recv()
    total = dxo[0]
    for k in range(2):
        total = total + yr[k].astype(F32)
    dx_out[...] = total.astype(BF)
    for p, cols in enumerate(ring1.slices):
        wq_out[:, cols] = ring1.finish(p)
    for copy in sink_z[5:]:
        copy.wait_recv()
    total = skz[0]
    for k in range(1, NZ):
        total = total + skz[k]
    sink_out[...] = total
    for p in range(2):
        wk_out[:, ring2.slices[p]] = ring2.finish(p)
        wv_out[:, ring2.slices[p]] = ring2.finish(p + 2)
    for copy in started:
        copy.wait_send()


def finish(*refs):
    for source, target in zip(refs[:5], refs[6:11]):
        target[...] = source[...]
    refs[11][...] = refs[5][0:1, 0:4]


def per_device(
    layer_input, output_grad, query_weight, key_weight, value_weight, out_weight, sink_logit
):
    vmem = pltpu.VMEM
    outside = pl.BlockSpec(memory_space=pltpu.HBM)
    inside = pl.BlockSpec(memory_space=pltpu.VMEM)
    results = (
        jax.ShapeDtypeStruct((TOK, 1024), BF),
        jax.ShapeDtypeStruct((64, QC), F32),
        jax.ShapeDtypeStruct((64, KC), F32),
        jax.ShapeDtypeStruct((64, KC), F32),
        jax.ShapeDtypeStruct((64, QC), F32),
    )
    outs = pl.pallas_call(
        kernel,
        name="attention_backward",
        out_shape=results + (jax.ShapeDtypeStruct((8, 128), F32),),
        in_specs=[outside] * 6 + [pl.BlockSpec(memory_space=pltpu.SMEM)],
        out_specs=[inside] * 6,
        scratch_shapes=[
            vmem((NY, 2, 4, TOK, 128), BF),
            vmem((NY, 2, 4, TOK, 128), BF),
            vmem((NY, 2, NX, TOK, 128), BF),
            vmem((NY, 2, NX, TOK, 128), BF),
        vmem((NY, 2, 128, NX * TOK), BF),
        vmem((NY, 2, 128, NX * TOK), BF),
            vmem((4096, QC), BF),
            vmem((4096, KC), BF),
            vmem((4096, KC), BF),
            vmem((QC, 4096), BF),
            vmem((TOK, QC + 2 * KC), F32),
            vmem((TOK, QC), F32),
            vmem((BAND, 2 * KC), BF),
            vmem((TOK, QC), BF),
            vmem((TOK, QC), BF),
            vmem((2, 2 * TOK, BAND), F32),
            vmem((2, 2 * TOK, 1), F32),
        vmem((2 * TOK, BAND), F32),
            vmem((3, 4, NX, TOK, 128), BF),
            vmem((BAND, 2 * KC), F32),
            vmem((2, WINDOW, 2 * KC), BF),
            vmem((2, WINDOW, 2 * KC), BF),
            vmem((3, NY, 2, 64, QC), F32),
            vmem((3, NY, 2, 64, QC), BF),
            vmem((3, NY, 2, 64, QC), BF),
            vmem((3, 2, 4, 64, QC), BF),
            vmem((3, 2, 4, 64, QC), BF),
            vmem((3, TOK, 1024), BF),
            vmem((2, TOK, 1024), BF),
        vmem((2, TOK // 2, 1024), BF),
            vmem((NY, TOK, 1024), F32),
            vmem((NX, 8, 128), F32),
            vmem((NC, 8, 128), F32),
            vmem((NZ, 8, 128), F32),
            pltpu.SemaphoreType.DMA((20,)),
            pltpu.SemaphoreType.DMA((COPIES,)),
            pltpu.SemaphoreType.DMA((COPIES,)),
        ],
        compiler_params=pltpu.CompilerParams(
            collective_id=0, has_side_effects=True, vmem_limit_bytes=53 * 1024 * 1024
        ),
    )(layer_input, output_grad, query_weight, key_weight, value_weight, out_weight, sink_logit)
    outs = pl.pallas_call(
        finish,
        name="finish",
        out_shape=results + (jax.ShapeDtypeStruct((1, 4), F32),),
        in_specs=[inside] * 6,
        out_specs=[inside] * 6,
        compiler_params=pltpu.CompilerParams(vmem_limit_bytes=8 * 1024 * 1024),
    )(*outs)
    return outs[:4] + (outs[4].T, outs[5].reshape(4))


def solution(mesh):
    placed = (
        P("sp", "tp"),
        P("sp", "tp"),
        P(None, "tp"),
        P(None, "tp"),
        P(None, "tp"),
        P("tp", None),
        P("tp"),
    )
    return jax.shard_map(
        per_device,
        mesh=mesh,
        in_specs=placed,
        out_specs=(
            P("sp", "tp"),
            P("sp", "tp"),
            P("sp", "tp"),
            P("sp", "tp"),
            P("tp", "sp"),
            P("tp"),
        ),
        check_vma=False,
    )
```
